256 devices in a mesh: dp: 4 (over x), kv: 32 (over z, y), tp: 2 (over core).
Axes of the slice: x: 4, y: 4, z: 8, core: 2. Of those that a mesh axis runs over, the one named last changes fastest.
Arguments:
- tokens: bfloat16 [4, 16, 2048], P('dp', None, 'kv'), may hold values from -18 to 18, as said below
- norm_gain: float32 [2048], P('kv'), may hold values from 0.1 to 1.9
- w_query: bfloat16 [2048, 3072], P('kv', 'tp'), may hold values from -0.125 to 0.125
- w_key: bfloat16 [2048, 3072], P('kv', 'tp'), may hold values from -0.125 to 0.125
- w_value: bfloat16 [2048, 3072], P('kv', 'tp'), may hold values from -0.125 to 0.125
- w_gate: bfloat16 [2048, 3072], P('kv', 'tp'), may hold values from -0.125 to 0.125
- w_out: bfloat16 [3072, 2048], P('tp', 'kv'), may hold values from -0.109375 to 0.109375
- head_bias: float32 [24], P('tp'), may hold values from -14 to -2
- cache_keys: bfloat16 [4, 16384, 24, 128], P('dp', 'kv', 'tp'), may hold values from -18 to 18, as said below
- cache_values: bfloat16 [4, 16384, 24, 128], P('dp', 'kv', 'tp'), may hold values from -6 to 6
- prefix_len: int32 [4], P('dp'), may hold values from 12288 to 16364
- accepted: int32 [4], P('dp'), may hold values from 1 to 4
- parent: int32 [4, 16], P('dp'), may hold values from -1 to 14, as said below
Outputs:
- mixed: bfloat16 [4, 16, 2048], P('dp', None, 'kv')
- keys_next: bfloat16 [4, 16384, 24, 128], P('dp', 'kv', 'tp')
- values_next: bfloat16 [4, 16384, 24, 128], P('dp', 'kv', 'tp')
The draws below stay inside these ranges and needn't reach their ends.
Inputs may be any that keep to these rules, and one draw needn't show every extreme that they name: `tokens`: entries of order one. `cache_keys`: entries of order one. parent of proposal 0 is -1; for p of 1 or more, parent[p] lies in max(p - 3, 0) to p - 1.
All inputs are finite; a program needn't handle non-finite values.
Results may differ from the reference program's by a relative error of at most 0.012.
Values may be sent and summed in bfloat16 or wider, within the bound.
No kernel may reach another device: no remote copies, remote signals or barrier semaphores. Data moves between devices by JAX's collectives and lax.ppermute only.
A program may use at most 64 MiB of HBM per device.

```python
import math
import jax
import jax.numpy as jnp
from jax import lax

D = 2048
HEADS = 24
HEAD = 128
BRANCH = 3072
PROPS = 16
LAST = 4
CTX = 16384
SEQS = 4
N_TP = 2


def draw_tokens(key, part):
    plain = jnp.clip(jax.random.normal(jax.random.fold_in(key, 11), (SEQS, PROPS, D), jnp.float32), -6.0, 6.0)
    blocks = (D + 63) // 64
    spread = jnp.exp(jax.random.uniform(jax.random.fold_in(key, 12), (1, 1, blocks), jnp.float32, math.log(0.3), math.log(3.0)))
    spread = jnp.repeat(spread, 64, axis=2)[:, :, :D]
    return (plain * spread).astype(jnp.bfloat16)


def draw_head_bias(key, part):
    lowest, highest = (-12.0, -2.0)
    return jax.random.uniform(jax.random.fold_in(key, 21), (HEADS,), jnp.float32, lowest, highest)


def draw_cache_keys(key, part):
    plain = jnp.clip(jax.random.normal(jax.random.fold_in(key, 31), (SEQS, CTX, HEADS, HEAD), jnp.float32), -6.0, 6.0)
    blocks = (CTX + 127) // 128
    spread = jnp.exp(jax.random.uniform(jax.random.fold_in(key, 32), (SEQS, blocks, HEADS, 1), jnp.float32, math.log(0.4), math.log(3.0)))
    spread = jnp.repeat(spread, 128, axis=1)[:, :CTX]
    return (plain * spread).astype(jnp.bfloat16)


def draw_parent(key, part):
    places = jnp.arange(PROPS, dtype=jnp.int32)
    back = jax.random.randint(jax.random.fold_in(key, 41), (SEQS, PROPS), 0, 3).astype(jnp.int32)
    chosen = jnp.maximum(places[None, :] - 1 - back, 0)
    return jnp.where(places[None, :] == 0, -1, chosen).astype(jnp.int32)


def set_ends(result, stream_key, smallest, high):
    shape = result.shape
    spot = [jax.random.randint(jax.random.fold_in(stream_key, axis), (), 0, shape[axis]) for axis in range(len(shape))]
    result = result.at[tuple(spot)].set(smallest)
    longest = shape.index(max(shape))
    spot[longest] = (spot[longest] + 1) % shape[longest]
    return result.at[tuple(spot)].set(high)


def levels(own_key, dims, cuts, least, top_value):
    factor_of, own = 1.0, jax.random.fold_in(own_key, 6)
    for position, parts in cuts:
        heights = jnp.exp(jax.random.uniform(jax.random.fold_in(own, position), (parts,), jnp.float32, least / len(cuts), top_value / len(cuts)))
        factor_of = factor_of * jnp.repeat(heights, dims[position] // parts).reshape([-1 if axis == position else 1 for axis in range(len(dims))])
    return factor_of


def gaussian(stream_key, shape, deviation, limit, shards=(), held_as=jnp.bfloat16):
    factor_of = levels(stream_key, shape, shards, -0.22, 0.18) if shards else 1.0
    values = jax.random.normal(stream_key, shape, jnp.float32) * deviation * factor_of
    return jnp.minimum(jnp.maximum(values, -limit), limit).astype(held_as)


def setup_inputs(seed: int = 0) -> dict:
    arg_keys = jax.random.split(jax.random.key(seed), 14)
    return {
        "tokens": draw_tokens(jax.random.fold_in(arg_keys[13], 71), 0),
        "norm_gain": jnp.clip(1.0 + 0.18 * jax.random.normal(arg_keys[1], (D,), jnp.float32), 0.1, 1.9),
        "w_query": gaussian(arg_keys[2], (D, BRANCH), D ** -0.5, 0.125, ((0, 32), (1, 2))),
        "w_key": gaussian(arg_keys[3], (D, BRANCH), D ** -0.5, 0.125, ((0, 32), (1, 2))),
        "w_value": gaussian(arg_keys[4], (D, BRANCH), D ** -0.5, 0.125, ((0, 32), (1, 2))),
        "w_gate": gaussian(arg_keys[5], (D, BRANCH), D ** -0.5, 0.125, ((0, 32), (1, 2))),
        "w_out": gaussian(arg_keys[6], (BRANCH, D), BRANCH ** -0.5, 0.109375, ((0, 2), (1, 32))),
        "head_bias": draw_head_bias(jax.random.fold_in(arg_keys[13], 71), 0),
        "cache_keys": draw_cache_keys(jax.random.fold_in(arg_keys[13], 71), 0),
        "cache_values": gaussian(arg_keys[9], (SEQS, CTX, HEADS, HEAD), 1.0, 6.0, ((0, 4), (1, 32), (2, 2))),
        "prefix_len": set_ends(jax.random.randint(arg_keys[10], (SEQS,), CTX - CTX // 4, CTX - PROPS - LAST + 1), jax.random.fold_in(arg_keys[10], 1), CTX - CTX // 4, CTX - PROPS - LAST).astype(jnp.int32),
        "accepted": set_ends(jax.random.randint(arg_keys[11], (SEQS,), 1, LAST + 1), jax.random.fold_in(arg_keys[11], 1), 1, LAST).astype(jnp.int32),
        "parent": draw_parent(jax.random.fold_in(arg_keys[13], 71), 0),
    }


EPS = 1e-06

def ancestry(parent):
    count = parent.shape[0]
    places = jnp.arange(count, dtype=jnp.int32)
    reach = (parent[:, None] == places[None, :]).astype(jnp.float32)
    for repeat in range(count.bit_length()):
        reach = jnp.minimum(reach + jnp.dot(reach, reach, precision=lax.Precision.HIGHEST), 1.0)
    return reach > 0.5

def one_sequence(packed, head_bias):
    query, key_new, value_new, cache_k, cache_v, valid, parent = packed
    factor = HEAD ** (-0.5)
    bias_col = head_bias[:, None, None]
    scores = jnp.einsum('phd,chd->hpc', query.astype(jnp.float32), cache_k.astype(jnp.float32)) * factor + bias_col
    live = (jnp.arange(cache_k.shape[0], dtype=jnp.int32) < valid)[None, None, :]
    keep_log = jnp.where(live, jax.nn.log_sigmoid(-scores), 0.0)
    family = ancestry(parent)[None]
    tree_scores = jnp.einsum('phd,jhd->hpj', query.astype(jnp.float32), key_new.astype(jnp.float32)) * factor + bias_col
    tree_keep = jnp.where(family, jax.nn.log_sigmoid(-tree_scores), 0.0)
    tail = lax.optimization_barrier(jnp.sum(tree_keep, axis=2, keepdims=True))
    later_cache = lax.cumsum(keep_log, axis=2, reverse=True) - keep_log + tail
    later_tree = lax.cumsum(tree_keep, axis=2, reverse=True) - tree_keep
    cache_weight = jnp.where(live, jnp.exp(jax.nn.log_sigmoid(scores) + later_cache), 0.0).astype(jnp.bfloat16)
    tree_weight = jnp.where(family, jnp.exp(jax.nn.log_sigmoid(tree_scores) + later_tree), 0.0).astype(jnp.bfloat16)
    attended = jnp.einsum('hpc,chd->phd', cache_weight.astype(jnp.float32), cache_v.astype(jnp.float32))
    attended = attended + jnp.einsum('hpj,jhd->phd', tree_weight.astype(jnp.float32), value_new.astype(jnp.float32))
    start = (valid.astype(jnp.int32), jnp.int32(0), jnp.int32(0))
    keys_next = lax.dynamic_update_slice(cache_k, key_new, start)
    values_next = lax.dynamic_update_slice(cache_v, value_new, start)
    return (attended, keys_next, values_next)

def reference(tokens, norm_gain, w_query, w_key, w_value, w_gate, w_out, head_bias, cache_keys, cache_values, prefix_len, accepted, parent):
    seqs, props, columns = tokens.shape
    flat = tokens.astype(jnp.float32).reshape(seqs * props, columns)
    squares = lax.optimization_barrier(jnp.sum(flat * flat, axis=1, keepdims=True))
    scaled = (flat * norm_gain).astype(jnp.bfloat16)
    rscale = lax.rsqrt(squares / columns + EPS)

    def project(weight):
        return (jnp.dot(scaled, weight, preferred_element_type=jnp.float32) * rscale).astype(jnp.bfloat16)
    query = project(w_query).reshape(seqs, props, HEADS, HEAD)
    key_new = project(w_key).reshape(seqs, props, HEADS, HEAD)
    value_new = project(w_value).reshape(seqs, props, HEADS, HEAD)
    gate = project(w_gate).astype(jnp.float32)
    valid = (prefix_len + accepted).astype(jnp.int32)
    attended, keys_next, values_next = lax.map(lambda packed: one_sequence(packed, head_bias), (query, key_new, value_new, cache_keys, cache_values, valid, parent))
    mixin = (attended.reshape(seqs * props, HEADS * HEAD) * jax.nn.silu(gate)).astype(jnp.bfloat16)
    group = HEADS * HEAD // N_TP
    total = jnp.zeros((seqs * props, columns), jnp.float32)
    for index in range(N_TP):
        part_out = jnp.dot(mixin[:, index * group:(index + 1) * group], w_out[index * group:(index + 1) * group], preferred_element_type=jnp.float32).astype(jnp.bfloat16)
        total = total + lax.optimization_barrier(part_out).astype(jnp.float32)
    mixed = total.astype(jnp.bfloat16).reshape(seqs, props, columns)
    return (mixed, keys_next, values_next)
```

```python
import jax
import jax.numpy as jnp
from jax import lax
from jax.sharding import PartitionSpec as P

D = 2048
HEAD = 128
EPS = 1e-06
INNER = 8


def groups_of(count):
    outer = count // INNER
    inner_groups = [[a * INNER + i for i in range(INNER)] for a in range(outer)]
    outer_groups = [[a * INNER + i for a in range(outer)] for i in range(INNER)]
    return inner_groups, outer_groups


def exchange(pieces, groups):
    return lax.all_to_all(pieces, "kv", 0, 0, axis_index_groups=groups, tiled=True)


def to_all(value, groups):
    return exchange(jnp.broadcast_to(value[None], (len(groups[0]), *value.shape)), groups)


def in_three(value):
    high = lax.reduce_precision(value, 8, 7)
    rest = value - high
    middle = lax.reduce_precision(rest, 8, 7)
    return jnp.concatenate([high, middle, rest - middle], axis=-1).astype(jnp.bfloat16)


def from_three(value, count):
    value = value[..., : 3 * count].astype(jnp.float32)
    return value[..., :count] + value[..., count : 2 * count] + value[..., 2 * count :]


def block(value, rows):
    return jnp.pad(value, ((0, rows - value.shape[0]), (0, HEAD - value.shape[1])))


def ancestry(parent):
    count = parent.shape[-1]
    places = jnp.arange(count, dtype=jnp.int32)
    reach = (parent[:, None] == places[None, :]).astype(jnp.float32)
    for repeat in range(count.bit_length()):
        reach = jnp.minimum(reach + jnp.dot(reach, reach), 1.0)
    return reach > 0.5


def sum_after(values):
    count = values.shape[-1]
    places = jnp.arange(count, dtype=jnp.int32)
    table = (places[:, None] > places[None, :]).astype(jnp.bfloat16)
    flat = values.reshape(-1, count)
    total = 0.0
    for piece in range(3):
        part = lax.reduce_precision(flat, 8, 7)
        flat = flat - part
        total = total + jnp.dot(
            part.astype(jnp.bfloat16), table, preferred_element_type=jnp.float32
        )
    return total.reshape(values.shape)


def log_sigmoids(scores):
    soft = jnp.log1p(jnp.exp(-jnp.abs(scores)))
    return jnp.minimum(scores, 0.0) - soft, jnp.minimum(-scores, 0.0) - soft


def merged(values, rests, extra):
    total = 0.0
    beyond = extra
    for index in reversed(range(values.shape[0])):
        total = total + jnp.exp(beyond)[..., None] * values[index].astype(jnp.float32)
        beyond = beyond + rests[index]
    return total, beyond


def local(
    tokens,
    norm_gain,
    w_query,
    w_key,
    w_value,
    w_gate,
    w_out,
    head_bias,
    cache_keys,
    cache_values,
    prefix_len,
    accepted,
    parent,
):
    inner_groups, outer_groups = groups_of(lax.axis_size("kv"))
    spot = lax.axis_index("kv")
    _, props, columns = tokens.shape
    heads = w_query.shape[1] // HEAD
    rows = heads * props
    share = 3 * rows // INNER
    flat = tokens[0].astype(jnp.float32)
    square_part = jnp.sum(flat * flat, axis=1)
    scaled = (flat * norm_gain).astype(jnp.bfloat16)
    parts = [
        jnp.einsum(
            "pk,khd->hpd",
            scaled,
            weight.reshape(columns, heads, HEAD),
            preferred_element_type=jnp.float32,
        ).astype(jnp.bfloat16).reshape(rows, HEAD)
        for weight in (w_query, w_key, w_value, w_gate)
    ]
    wide = lambda value: jnp.broadcast_to(value[None], (INNER, *value.shape))
    pieces = jnp.concatenate(
        [
            wide(parts[0]),
            jnp.concatenate(parts[1:], axis=0).reshape(INNER, share, HEAD),
            wide(block(in_three(square_part[None]), 8)),
        ],
        axis=1,
    )
    total = exchange(pieces, inner_groups).astype(jnp.float32).sum(axis=0)
    squares = from_three(total[rows + share], props)
    pieces = jnp.concatenate(
        [total[: rows + share].astype(jnp.bfloat16), block(in_three(squares[None]), 8)], axis=0
    )
    total = to_all(pieces, outer_groups).astype(jnp.float32).sum(axis=0)
    squares = from_three(total[rows + share], props)
    rscale = lax.rsqrt(squares / D + EPS)
    query = (
        (total[:rows].reshape(heads, props, HEAD) * rscale[None, :, None]).astype(jnp.bfloat16)
    )
    turned = jnp.where((spot * share) % props == 0, rscale, jnp.roll(rscale, props // 2))
    turned = jnp.tile(turned, -(-share // props))[:share]
    own_share = (total[rows : rows + share] * turned[:, None]).astype(jnp.bfloat16)

    factor = HEAD ** (-0.5)
    bias_col = head_bias[:, None, None]
    ctx_dev = cache_keys.shape[1]
    valid = (prefix_len + accepted)[0]
    places = spot * ctx_dev + jnp.arange(ctx_dev, dtype=jnp.int32)
    live = (places < valid)[None, None, :]
    scores = (
        jnp.einsum("hpd,chd->hpc", query, cache_keys[0], preferred_element_type=jnp.float32)
        * factor
        + bias_col
    )
    take_log, keep_log = log_sigmoids(scores)
    keep_log = jnp.where(live, keep_log, 0.0)
    rest = jnp.sum(keep_log, axis=2)
    weight = jnp.where(live, jnp.exp(take_log + sum_after(keep_log)), 0.0).astype(jnp.bfloat16)
    local_sum = jnp.einsum(
        "hpc,chd->hpd", weight, cache_values[0], preferred_element_type=jnp.float32
    )
    pieces = jnp.concatenate(
        [
            local_sum.astype(jnp.bfloat16).reshape(rows, HEAD),
            own_share,
            block(in_three(rest), 16),
        ],
        axis=0,
    )
    arrived = to_all(pieces, inner_groups)
    value_sum, rest = merged(
        arrived[:, :rows].reshape(INNER, heads, props, HEAD),
        from_three(arrived[:, rows + share : rows + share + heads], props),
        jnp.zeros((heads, props), jnp.float32),
    )
    shares = arrived[:, rows : rows + share].reshape(3, heads, props, HEAD)
    pieces = jnp.concatenate(
        [value_sum.astype(jnp.bfloat16).reshape(rows, HEAD), block(in_three(rest), 16)], axis=0
    )
    arrived = to_all(pieces, outer_groups)
    key_new, value_new, gate = shares[0], shares[1], shares[2]

    family = ancestry(parent[0])[None]
    tree_scores = (
        jnp.einsum("hpd,hjd->hpj", query, key_new, preferred_element_type=jnp.float32) * factor
        + bias_col
    )
    tree_take, tree_keep = log_sigmoids(tree_scores)
    tree_keep = jnp.where(family, tree_keep, 0.0)
    tail = jnp.sum(tree_keep, axis=2)
    tree_weight = jnp.where(family, jnp.exp(tree_take + sum_after(tree_keep)), 0.0).astype(
        jnp.bfloat16
    )
    tree_part = jnp.einsum(
        "hpj,hjd->hpd", tree_weight, value_new, preferred_element_type=jnp.float32
    )
    opened = jax.nn.silu(gate.astype(jnp.float32))

    attended, _ = merged(
        arrived[:, :rows].reshape(len(outer_groups[0]), heads, props, HEAD),
        from_three(arrived[:, rows : rows + heads], props),
        tail,
    )
    mixin = ((attended + tree_part) * opened).astype(jnp.bfloat16)
    part_out = jnp.einsum(
        "hpd,hdo->po",
        mixin,
        w_out.reshape(heads, HEAD, w_out.shape[1]),
        preferred_element_type=jnp.float32,
    ).astype(jnp.bfloat16)
    both = lax.all_gather(part_out, "tp").astype(jnp.float32)
    mixed = both.sum(0).astype(jnp.bfloat16)[None]

    offset = valid - spot * ctx_dev
    start = jnp.clip(offset, 0, ctx_dev - props)
    source = jnp.arange(props, dtype=jnp.int32) + start - offset
    picker = (source[:, None] == jnp.arange(props, dtype=jnp.int32)[None, :]).astype(jnp.bfloat16)
    inside = ((source >= 0) & (source < props))[None, :, None, None]

    def written(cache, fresh):
        placed = jnp.einsum(
            "rp,hpd->rhd", picker, fresh, preferred_element_type=jnp.float32
        ).astype(jnp.bfloat16)[None]
        there = lax.dynamic_slice(cache, (0, start, 0, 0), (1, props, heads, HEAD))
        return lax.dynamic_update_slice(cache, jnp.where(inside, placed, there), (0, start, 0, 0))

    return (mixed, written(cache_keys, key_new), written(cache_values, value_new))


def solution(mesh):
    return jax.shard_map(
        local,
        mesh=mesh,
        in_specs=(
            P("dp", None, "kv"),
            P("kv"),
            P("kv", "tp"),
            P("kv", "tp"),
            P("kv", "tp"),
            P("kv", "tp"),
            P("tp", "kv"),
            P("tp"),
            P("dp", "kv", "tp", None),
            P("dp", "kv", "tp", None),
            P("dp"),
            P("dp"),
            P("dp", None),
        ),
        out_specs=(P("dp", None, "kv"), P("dp", "kv", "tp", None), P("dp", "kv", "tp", None)),
        check_vma=False,
    )
```

```python
import jax
import jax.numpy as jnp
from jax import lax
from jax.experimental import pallas as pl
from jax.experimental.pallas import tpu as pltpu
from jax.sharding import PartitionSpec as P

D = 2048
HEAD = 128
EPS = 1e-06
INNER = 8
PROPS = 16
WINDOW = 32
F32 = jnp.float32
BF16 = jnp.bfloat16
VMEM = pl.BlockSpec(memory_space=pltpu.VMEM)
SMEM = pl.BlockSpec(memory_space=pltpu.SMEM)
ANY = pl.BlockSpec(memory_space=pl.ANY)


def groups_of(count):
    outer = count // INNER
    inner_groups = [[a * INNER + i for i in range(INNER)] for a in range(outer)]
    outer_groups = [[a * INNER + i for a in range(outer)] for i in range(INNER)]
    return inner_groups, outer_groups


def exchange(pieces, groups):
    return lax.all_to_all(pieces, "kv", 0, 0, axis_index_groups=groups, tiled=True)


def iota(shape, dim):
    return lax.broadcasted_iota(jnp.int32, shape, dim)


def in_three(value):
    high = value.astype(BF16).astype(F32)
    rest = value - high
    middle = rest.astype(BF16).astype(F32)
    return high, middle, rest - middle


def dot(left, right):
    return jnp.dot(left, right, preferred_element_type=F32)


def dot_t(left, right):
    return lax.dot_general(left, right, (((1,), (1,)), ((), ())), preferred_element_type=F32)


def log_sigmoids(scores):
    soft = jnp.log1p(jnp.exp(-jnp.abs(scores)))
    return jnp.minimum(scores, 0.0) - soft, jnp.minimum(-scores, 0.0) - soft


def square_block(squares):
    lane = iota((PROPS, HEAD), 1)
    block = jnp.zeros((PROPS, HEAD), F32)
    for index, piece in enumerate(in_three(squares)):
        block = jnp.where(lane == index, piece, block)
    return block.astype(BF16)


def rest_block(rests):
    lane = iota((PROPS, HEAD), 1)
    block = jnp.zeros((PROPS, HEAD), F32)
    for index, rest in enumerate(rests):
        block = jnp.where(lane == index, rest, block)
    high, middle, low = in_three(block)
    block = high + pltpu.roll(middle, PROPS, 1) + pltpu.roll(low, 2 * PROPS, 1)
    return block.astype(BF16)


def rest_sums(block):
    block = block.astype(F32)
    return block + pltpu.roll(block, HEAD - PROPS, 1) + pltpu.roll(block, HEAD - 2 * PROPS, 1)


def after_table(width):
    row = iota((width, 2 * HEAD), 0)
    column = iota((width, 2 * HEAD), 1)
    return jnp.where((row > column) | (column >= HEAD), 1.0, 0.0).astype(BF16)


def after_and_all(values, table):
    high = values.astype(BF16)
    rest = values - high.astype(F32)
    middle = rest.astype(BF16)
    low = (rest - middle.astype(F32)).astype(BF16)
    sums = dot(high, table) + dot(middle, table) + dot(low, table)
    return sums[:, :HEAD], sums[:, HEAD:]


def project_kernel(tokens, gain, w_query, w_key, w_value, w_gate, out):
    heads = w_query.shape[1] // HEAD
    rows = heads * PROPS
    share = out.shape[1] - rows - PROPS
    flat = tokens[...].astype(F32)
    block = square_block(jnp.sum(flat * flat, axis=1, keepdims=True))
    scaled = (flat * gain[...]).astype(BF16)
    query = dot(scaled, w_query[...]).astype(BF16)
    for dest in range(INNER):
        for head in range(heads):
            out[dest, head * PROPS : (head + 1) * PROPS, :] = query[
                :, head * HEAD : (head + 1) * HEAD
            ]
        out[dest, rows + share :, :] = block
    slots = share // PROPS
    for which, weight in enumerate((w_key, w_value, w_gate)):
        part = dot(scaled, weight[...]).astype(BF16)
        for head in range(heads):
            dest, slot = divmod(which * heads + head, slots)
            out[dest, rows + slot * PROPS : rows + (slot + 1) * PROPS, :] = part[
                :, head * HEAD : (head + 1) * HEAD
            ]
    for spare in range(3 * heads, INNER * slots):
        dest, slot = divmod(spare, slots)
        out[dest, rows + slot * PROPS : rows + (slot + 1) * PROPS, :] = jnp.zeros(
            (PROPS, HEAD), BF16
        )


def add_up(arrived):
    total = arrived[0].astype(F32)
    for index in range(1, arrived.shape[0]):
        total = total + arrived[index].astype(F32)
    return total


def forward_kernel(arrived, out):
    count = arrived.shape[1] - PROPS
    total = add_up(arrived)
    sums = total[:count].astype(BF16)
    block = square_block(jnp.sum(total[count:], axis=1, keepdims=True))
    for dest in range(out.shape[0]):
        out[dest, :count, :] = sums
        out[dest, count:, :] = block


def attend_kernel(
    scalars,
    arrived,
    bias,
    keys,
    values,
    out,
    query_out,
    keys_next,
    values_next,
    keys_window,
    values_window,
    sems,
):
    heads, ctx_dev, _ = keys.shape
    rows = heads * PROPS
    copies = [
        pltpu.make_async_copy(keys, keys_next, sems.at[0]),
        pltpu.make_async_copy(values, values_next, sems.at[1]),
    ]
    for copy in copies:
        copy.start()
    offset = scalars[0]
    first = pl.multiple_of(scalars[1], PROPS)
    total = add_up(arrived)
    squares = jnp.sum(total[arrived.shape[1] - PROPS :], axis=1, keepdims=True)
    rscale = lax.rsqrt(squares / D + EPS)
    share = arrived.shape[1] - PROPS - rows
    for slot in range(share // PROPS):
        there = slice(rows + slot * PROPS, rows + (slot + 1) * PROPS)
        piece = (total[there] * rscale).astype(BF16)
        for dest in range(INNER):
            out[dest, there, :] = piece
    factor = HEAD ** (-0.5)
    live = iota((PROPS, ctx_dev), 1) < offset
    takes, keeps = [], []
    for head in range(heads):
        there = slice(head * PROPS, (head + 1) * PROPS)
        query = (total[there] * rscale).astype(BF16)
        query_out[there, :] = query
        scores = dot_t(query, keys[head]) * factor + bias[head : head + 1, :]
        take, keep = log_sigmoids(scores)
        takes.append(take)
        keeps.append(jnp.where(live, keep, 0.0))
    keep = jnp.concatenate(keeps, axis=0)
    table = after_table(HEAD)
    beyond = jnp.zeros((rows, HEAD), F32)
    laters = []
    for chunk in reversed(range(ctx_dev // HEAD)):
        inside, whole = after_and_all(keep[:, chunk * HEAD : (chunk + 1) * HEAD], table)
        laters.append(inside + beyond)
        beyond = beyond + whole
    later = jnp.concatenate(laters[::-1], axis=1)
    rests = []
    for head in range(heads):
        there = slice(head * PROPS, (head + 1) * PROPS)
        weight = jnp.where(live, jnp.exp(takes[head] + later[there]), 0.0).astype(BF16)
        summed = dot(weight, values[head]).astype(BF16)
        for dest in range(INNER):
            out[dest, there, :] = summed
        rests.append(beyond[there])
    block = rest_block(rests)
    for dest in range(INNER):
        out[dest, rows + share :, :] = block
    keys_window[...] = keys[:, pl.ds(first, WINDOW), :]
    values_window[...] = values[:, pl.ds(first, WINDOW), :]
    for copy in copies:
        copy.wait()


def merge_kernel(arrived, out, fresh):
    count = arrived.shape[0]
    rows = out.shape[1] - PROPS
    heads = rows // PROPS
    share = arrived.shape[1] - PROPS - rows
    for source in range(count):
        fresh[source * share : (source + 1) * share, :] = arrived[source, rows : rows + share, :]
    beyond = jnp.zeros((PROPS, HEAD), F32)
    factors = []
    for source in reversed(range(count)):
        factors.append(jnp.exp(beyond))
        beyond = beyond + rest_sums(arrived[source, rows + share :, :])
    factors = factors[::-1]
    for head in range(heads):
        there = slice(head * PROPS, (head + 1) * PROPS)
        total = jnp.zeros((PROPS, HEAD), F32)
        for source in range(count):
            total = total + factors[source][:, head : head + 1] * arrived[
                source, there, :
            ].astype(F32)
        total = total.astype(BF16)
        for dest in range(out.shape[0]):
            out[dest, there, :] = total
    block = rest_block([beyond[:, head : head + 1] for head in range(heads)])
    for dest in range(out.shape[0]):
        out[dest, rows:, :] = block


def finish_kernel(
    scalars,
    parent,
    arrived,
    fresh,
    query,
    bias,
    w_out,
    keys_window,
    values_window,
    keys_old,
    values_old,
    out,
    keys_next,
    values_next,
    mixin,
    patches,
    masks,
    sems,
):
    del keys_old, values_old
    count = arrived.shape[0]
    rows = arrived.shape[1] - PROPS
    heads = rows // PROPS
    offset = scalars[0]
    first = pl.multiple_of(scalars[1], PROPS)
    source = first + iota((WINDOW, PROPS), 0) - offset
    picker = jnp.where(source == iota((WINDOW, PROPS), 1), 1.0, 0.0).astype(BF16)
    source = first + iota((WINDOW, HEAD), 0) - offset
    inside = (source >= 0) & (source < PROPS)
    copies = []
    for which, (window, target) in enumerate(
        ((keys_window, keys_next), (values_window, values_next))
    ):
        patched = patches.at[which]
        for head in range(heads):
            start = (which * heads + head) * PROPS
            placed = dot(picker, fresh[start : start + PROPS, :])
            patches[which, head] = jnp.where(inside, placed, window[head].astype(F32)).astype(BF16)
        copies.append(
            pltpu.make_async_copy(patched, target.at[:, pl.ds(first, WINDOW), :], sems.at[which])
        )
        copies[-1].start()
    row = iota((PROPS, PROPS), 0)
    reach = jnp.zeros((PROPS, PROPS), jnp.int32)
    masks[0] = 0
    for index in range(1, PROPS):
        above = parent[index]
        mask = masks[above] | (1 << above)
        masks[index] = mask
        reach = jnp.where(row == index, mask, reach)
    family = ((reach >> iota((PROPS, PROPS), 1)) & 1) == 1
    factor = HEAD ** (-0.5)
    takes, keeps = [], []
    for head in range(heads):
        there = slice(head * PROPS, (head + 1) * PROPS)
        scores = dot_t(query[there, :], fresh[there, :]) * factor + bias[head : head + 1, :PROPS]
        take, keep = log_sigmoids(scores)
        takes.append(take)
        keeps.append(jnp.where(family, keep, 0.0))
    later, tail = after_and_all(jnp.concatenate(keeps, axis=0), after_table(PROPS))
    beyond = jnp.zeros((PROPS, HEAD), F32)
    beyonds = []
    for index in reversed(range(count)):
        beyonds.append(beyond)
        beyond = beyond + rest_sums(arrived[index, rows:, :])
    beyonds = beyonds[::-1]
    for head in range(heads):
        there = slice(head * PROPS, (head + 1) * PROPS)
        weight = jnp.where(family, jnp.exp(takes[head] + later[there, :PROPS]), 0.0).astype(BF16)
        start = (heads + head) * PROPS
        total = dot(weight, fresh[start : start + PROPS, :])
        for index in range(count):
            total = total + jnp.exp(beyonds[index][:, head : head + 1] + tail[there]) * arrived[
                index, there, :
            ].astype(F32)
        start = (2 * heads + head) * PROPS
        gate = fresh[start : start + PROPS, :].astype(F32)
        mixin[:, head * HEAD : (head + 1) * HEAD] = (total * (gate * jax.nn.sigmoid(gate))).astype(
            BF16
        )
    out[...] = dot_t(mixin[...], w_out[...]).astype(BF16)
    for copy in copies:
        copy.wait()


def shaped(dims, dtype=BF16):
    return jax.ShapeDtypeStruct(dims, dtype)


def local(
    tokens,
    norm_gain,
    w_query,
    w_key,
    w_value,
    w_gate,
    w_out,
    head_bias,
    cache_keys,
    cache_values,
    prefix_len,
    accepted,
    parent,
):
    inner_groups, outer_groups = groups_of(lax.axis_size("kv"))
    outer = len(outer_groups[0])
    spot = lax.axis_index("kv")
    heads = w_query.shape[1] // HEAD
    ctx_dev = cache_keys.shape[1]
    rows = heads * PROPS
    share = -(-3 * heads // INNER) * PROPS
    sent = rows + share + PROPS
    offset = (prefix_len + accepted)[0] - spot * ctx_dev
    first = jnp.clip(offset // PROPS * PROPS, 0, ctx_dev - WINDOW)
    scalars = jnp.stack([offset, first])
    bias = jnp.broadcast_to(head_bias[:, None], (heads, ctx_dev))
    keys = jnp.transpose(cache_keys[0], (1, 0, 2))
    values = jnp.transpose(cache_values[0], (1, 0, 2))

    pieces = pl.pallas_call(
        project_kernel,
        out_shape=shaped((INNER, sent, HEAD)),
        in_specs=[VMEM] * 6,
        out_specs=VMEM,
        name="project",
    )(tokens[0], norm_gain[None], w_query, w_key, w_value, w_gate)
    pieces = pl.pallas_call(
        forward_kernel,
        out_shape=shaped((outer, sent, HEAD)),
        in_specs=[VMEM],
        out_specs=VMEM,
        name="forward",
    )(exchange(pieces, inner_groups))
    window = shaped((heads, WINDOW, HEAD))
    pieces, query, keys_next, values_next, keys_window, values_window = pl.pallas_call(
        attend_kernel,
        out_shape=(
            shaped((INNER, sent, HEAD)),
            shaped((rows, HEAD)),
            shaped(keys.shape),
            shaped(values.shape),
            window,
            window,
        ),
        in_specs=[SMEM, VMEM, VMEM, VMEM, VMEM],
        out_specs=(VMEM, VMEM, ANY, ANY, VMEM, VMEM),
        scratch_shapes=[pltpu.SemaphoreType.DMA((2,))],
        name="attend",
    )(scalars, exchange(pieces, outer_groups), bias, keys, values)
    pieces, fresh = pl.pallas_call(
        merge_kernel,
        out_shape=(shaped((outer, rows + PROPS, HEAD)), shaped((INNER * share, HEAD))),
        in_specs=[VMEM],
        out_specs=(VMEM, VMEM),
        name="merge",
    )(exchange(pieces, inner_groups))
    part_out, keys_next, values_next = pl.pallas_call(
        finish_kernel,
        out_shape=(
            shaped((PROPS, w_out.shape[1])),
            shaped(keys.shape),
            shaped(values.shape),
        ),
        in_specs=[SMEM, SMEM] + [VMEM] * 7 + [ANY, ANY],
        out_specs=(VMEM, ANY, ANY),
        input_output_aliases={9: 1, 10: 2},
        scratch_shapes=[
            pltpu.VMEM((PROPS, heads * HEAD), BF16),
            pltpu.VMEM((2, heads, WINDOW, HEAD), BF16),
            pltpu.SMEM((PROPS,), jnp.int32),
            pltpu.SemaphoreType.DMA((2,)),
        ],
        name="finish",
    )(
        scalars,
        parent[0],
        exchange(pieces, outer_groups),
        fresh,
        query,
        bias,
        w_out.T,
        keys_window,
        values_window,
        keys_next,
        values_next,
    )
    both = lax.all_gather(part_out, "tp").astype(F32)
    mixed = both.sum(0).astype(BF16)[None]
    return (
        mixed,
        jnp.transpose(keys_next, (1, 0, 2))[None],
        jnp.transpose(values_next, (1, 0, 2))[None],
    )


def solution(mesh):
    return jax.shard_map(
        local,
        mesh=mesh,
        in_specs=(
            P("dp", None, "kv"),
            P("kv"),
            P("kv", "tp"),
            P("kv", "tp"),
            P("kv", "tp"),
            P("kv", "tp"),
            P("tp", "kv"),
            P("tp"),
            P("dp", "kv", "tp", None),
            P("dp", "kv", "tp", None),
            P("dp"),
            P("dp"),
            P("dp", None),
        ),
        out_specs=(P("dp", None, "kv"), P("dp", "kv", "tp", None), P("dp", "kv", "tp", None)),
        check_vma=False,
    )
```

```python
import jax
import jax.numpy as jnp
from jax import lax
from jax.experimental import pallas as pl
from jax.experimental.pallas import tpu as pltpu
from jax.sharding import PartitionSpec as P

D = 2048
HEAD = 128
EPS = 1e-06
INNER = 8
PROPS = 16
WINDOW = 32
F32 = jnp.float32
BF16 = jnp.bfloat16
VMEM = pl.BlockSpec(memory_space=pltpu.VMEM)
SMEM = pl.BlockSpec(memory_space=pltpu.SMEM)
ANY = pl.BlockSpec(memory_space=pl.ANY)
PARAMS = pltpu.CompilerParams(vmem_limit_bytes=16 * 2**20)


def groups_of(count):
    outer = count // INNER
    inner_groups = [[a * INNER + i for i in range(INNER)] for a in range(outer)]
    outer_groups = [[a * INNER + i for a in range(outer)] for i in range(INNER)]
    return inner_groups, outer_groups


def exchange(pieces, groups):
    return lax.all_to_all(pieces, "kv", 0, 0, axis_index_groups=groups, tiled=True)


def iota(shape, dim):
    return lax.broadcasted_iota(jnp.int32, shape, dim)


def in_three(value):
    high = value.astype(BF16).astype(F32)
    rest = value - high
    middle = rest.astype(BF16).astype(F32)
    return high, middle, rest - middle


def dot(left, right):
    return jnp.dot(left, right, preferred_element_type=F32)


def dot_t(left, right):
    return lax.dot_general(left, right, (((1,), (1,)), ((), ())), preferred_element_type=F32)


def log_sigmoids(scores):
    soft = jnp.log1p(jnp.exp(-jnp.abs(scores)))
    return jnp.minimum(scores, 0.0) - soft, jnp.minimum(-scores, 0.0) - soft


def square_block(squares):
    lane = iota((PROPS, HEAD), 1)
    block = jnp.zeros((PROPS, HEAD), F32)
    for index, piece in enumerate(in_three(squares)):
        block = jnp.where(lane == index, piece, block)
    return block.astype(BF16)


def rest_block(rests):
    lane = iota((PROPS, HEAD), 1)
    block = jnp.zeros((PROPS, HEAD), F32)
    for index, rest in enumerate(rests):
        block = jnp.where(lane == index, rest, block)
    high, middle, low = in_three(block)
    block = high + pltpu.roll(middle, PROPS, 1) + pltpu.roll(low, 2 * PROPS, 1)
    return block.astype(BF16)


def rest_sums(block):
    block = block.astype(F32)
    return block + pltpu.roll(block, HEAD - PROPS, 1) + pltpu.roll(block, HEAD - 2 * PROPS, 1)


def after_table(width):
    row = iota((width, 2 * HEAD), 0)
    column = iota((width, 2 * HEAD), 1)
    return jnp.where((row > column) | (column >= HEAD), 1.0, 0.0).astype(BF16)


def after_and_all(values, table):
    high = values.astype(BF16)
    rest = values - high.astype(F32)
    middle = rest.astype(BF16)
    low = (rest - middle.astype(F32)).astype(BF16)
    sums = dot(high, table) + dot(middle, table) + dot(low, table)
    return sums[:, :HEAD], sums[:, HEAD:]


def project_kernel(
    prefix_len,
    accepted,
    tokens_far,
    gain_far,
    query_far,
    key_far,
    value_far,
    gate_far,
    out,
    tokens,
    gain,
    w_query,
    w_key,
    w_value,
    w_gate,
    sems,
):
    del prefix_len, accepted
    copies = [
        pltpu.make_async_copy(source, target, sems.at[index])
        for index, (source, target) in enumerate(
            (
                (tokens_far, tokens),
                (gain_far, gain),
                (query_far, w_query),
                (key_far, w_key),
                (value_far, w_value),
                (gate_far, w_gate),
            )
        )
    ]
    for copy in copies:
        copy.start()
    heads = w_query.shape[1] // HEAD
    rows = heads * PROPS
    share = out.shape[1] - rows - PROPS
    copies[0].wait()
    flat = tokens[...].astype(F32)
    block = square_block(jnp.sum(flat * flat, axis=1, keepdims=True))
    copies[1].wait()
    scaled = (flat * gain[...]).astype(BF16)
    copies[2].wait()
    query = dot(scaled, w_query[...]).astype(BF16)
    for dest in range(INNER):
        for head in range(heads):
            out[dest, head * PROPS : (head + 1) * PROPS, :] = query[
                :, head * HEAD : (head + 1) * HEAD
            ]
        out[dest, rows + share :, :] = block
    slots = share // PROPS
    for which, weight in enumerate((w_key, w_value, w_gate)):
        copies[3 + which].wait()
        part = dot(scaled, weight[...]).astype(BF16)
        for head in range(heads):
            dest, slot = divmod(which * heads + head, slots)
            out[dest, rows + slot * PROPS : rows + (slot + 1) * PROPS, :] = part[
                :, head * HEAD : (head + 1) * HEAD
            ]
    for spare in range(3 * heads, INNER * slots):
        dest, slot = divmod(spare, slots)
        out[dest, rows + slot * PROPS : rows + (slot + 1) * PROPS, :] = jnp.zeros(
            (PROPS, HEAD), BF16
        )


def add_up(arrived):
    total = arrived[0].astype(F32)
    for index in range(1, arrived.shape[0]):
        total = total + arrived[index].astype(F32)
    return total


def forward_kernel(arrived, out):
    count = arrived.shape[1] - PROPS
    total = add_up(arrived)
    sums = total[:count].astype(BF16)
    block = square_block(jnp.sum(total[count:], axis=1, keepdims=True))
    for dest in range(out.shape[0]):
        out[dest, :count, :] = sums
        out[dest, count:, :] = block


def attend_kernel(
    prefix_len,
    accepted,
    bias,
    arrived,
    keys,
    values,
    out,
    query_out,
    keys_next,
    values_next,
    keys_window,
    values_window,
    sems,
):
    heads, ctx_dev, _ = keys.shape
    rows = heads * PROPS
    copies = [
        pltpu.make_async_copy(keys, keys_next, sems.at[0]),
        pltpu.make_async_copy(values, values_next, sems.at[1]),
    ]
    for copy in copies:
        copy.start()
    offset, first = window_of(prefix_len, accepted, ctx_dev)
    total = add_up(arrived)
    squares = jnp.sum(total[arrived.shape[1] - PROPS :], axis=1, keepdims=True)
    rscale = lax.rsqrt(squares / D + EPS)
    share = arrived.shape[1] - PROPS - rows
    for slot in range(share // PROPS):
        there = slice(rows + slot * PROPS, rows + (slot + 1) * PROPS)
        piece = (total[there] * rscale).astype(BF16)
        for dest in range(INNER):
            out[dest, there, :] = piece
    factor = HEAD ** (-0.5)
    live = iota((PROPS, ctx_dev), 1) < offset
    takes, keeps = [], []
    for head in range(heads):
        there = slice(head * PROPS, (head + 1) * PROPS)
        query = (total[there] * rscale).astype(BF16)
        query_out[there, :] = query
        scores = dot_t(query, keys[head]) * factor + bias[head]
        take, keep = log_sigmoids(scores)
        takes.append(take)
        keeps.append(jnp.where(live, keep, 0.0))
    keep = jnp.concatenate(keeps, axis=0)
    table = after_table(HEAD)
    beyond = jnp.zeros((rows, HEAD), F32)
    laters = []
    for chunk in reversed(range(ctx_dev // HEAD)):
        inside, whole = after_and_all(keep[:, chunk * HEAD : (chunk + 1) * HEAD], table)
        laters.append(inside + beyond)
        beyond = beyond + whole
    later = jnp.concatenate(laters[::-1], axis=1)
    rests = []
    for head in range(heads):
        there = slice(head * PROPS, (head + 1) * PROPS)
        weight = jnp.where(live, jnp.exp(takes[head] + later[there]), 0.0).astype(BF16)
        summed = dot(weight, values[head]).astype(BF16)
        for dest in range(INNER):
            out[dest, there, :] = summed
        rests.append(beyond[there])
    block = rest_block(rests)
    for dest in range(INNER):
        out[dest, rows + share :, :] = block
    keys_window[...] = keys[:, pl.ds(first, WINDOW), :]
    values_window[...] = values[:, pl.ds(first, WINDOW), :]
    for copy in copies:
        copy.wait()


def merge_kernel(arrived, out, fresh):
    count = arrived.shape[0]
    rows = out.shape[1] - PROPS
    heads = rows // PROPS
    share = arrived.shape[1] - PROPS - rows
    for source in range(count):
        fresh[source * share : (source + 1) * share, :] = arrived[source, rows : rows + share, :]
    beyond = jnp.zeros((PROPS, HEAD), F32)
    factors = []
    for source in reversed(range(count)):
        factors.append(jnp.exp(beyond))
        beyond = beyond + rest_sums(arrived[source, rows + share :, :])
    factors = factors[::-1]
    for head in range(heads):
        there = slice(head * PROPS, (head + 1) * PROPS)
        total = jnp.zeros((PROPS, HEAD), F32)
        for source in range(count):
            total = total + factors[source][:, head : head + 1] * arrived[
                source, there, :
            ].astype(F32)
        total = total.astype(BF16)
        for dest in range(out.shape[0]):
            out[dest, there, :] = total
    block = rest_block([beyond[:, head : head + 1] for head in range(heads)])
    for dest in range(out.shape[0]):
        out[dest, rows:, :] = block


def finish_kernel(
    prefix_len,
    accepted,
    bias,
    parent,
    arrived,
    fresh,
    query,
    w_out,
    keys_window,
    values_window,
    keys_old,
    values_old,
    out,
    keys_next,
    values_next,
    mixin,
    patches,
    masks,
    sems,
):
    del keys_old, values_old
    count = arrived.shape[0]
    rows = arrived.shape[1] - PROPS
    heads = rows // PROPS
    offset, first = window_of(prefix_len, accepted, keys_next.shape[1])
    source = first + iota((WINDOW, PROPS), 0) - offset
    picker = jnp.where(source == iota((WINDOW, PROPS), 1), 1.0, 0.0).astype(BF16)
    source = first + iota((WINDOW, HEAD), 0) - offset
    inside = (source >= 0) & (source < PROPS)
    copies = []
    for which, (window, target) in enumerate(
        ((keys_window, keys_next), (values_window, values_next))
    ):
        patched = patches.at[which]
        for head in range(heads):
            start = (which * heads + head) * PROPS
            placed = dot(picker, fresh[start : start + PROPS, :])
            patches[which, head] = jnp.where(inside, placed, window[head].astype(F32)).astype(BF16)
        copies.append(
            pltpu.make_async_copy(patched, target.at[:, pl.ds(first, WINDOW), :], sems.at[which])
        )
        copies[-1].start()
    row = iota((PROPS, PROPS), 0)
    reach = jnp.zeros((PROPS, PROPS), jnp.int32)
    masks[0] = 0
    for index in range(1, PROPS):
        above = parent[index]
        mask = masks[above] | (1 << above)
        masks[index] = mask
        reach = jnp.where(row == index, mask, reach)
    family = ((reach >> iota((PROPS, PROPS), 1)) & 1) == 1
    factor = HEAD ** (-0.5)
    takes, keeps = [], []
    for head in range(heads):
        there = slice(head * PROPS, (head + 1) * PROPS)
        scores = dot_t(query[there, :], fresh[there, :]) * factor + bias[head]
        take, keep = log_sigmoids(scores)
        takes.append(take)
        keeps.append(jnp.where(family, keep, 0.0))
    later, tail = after_and_all(jnp.concatenate(keeps, axis=0), after_table(PROPS))
    beyond = jnp.zeros((PROPS, HEAD), F32)
    beyonds = []
    for index in reversed(range(count)):
        beyonds.append(beyond)
        beyond = beyond + rest_sums(arrived[index, rows:, :])
    beyonds = beyonds[::-1]
    for head in range(heads):
        there = slice(head * PROPS, (head + 1) * PROPS)
        weight = jnp.where(family, jnp.exp(takes[head] + later[there, :PROPS]), 0.0).astype(BF16)
        start = (heads + head) * PROPS
        total = dot(weight, fresh[start : start + PROPS, :])
        for index in range(count):
            total = total + jnp.exp(beyonds[index][:, head : head + 1] + tail[there]) * arrived[
                index, there, :
            ].astype(F32)
        start = (2 * heads + head) * PROPS
        gate = fresh[start : start + PROPS, :].astype(F32)
        mixin[:, head * HEAD : (head + 1) * HEAD] = (total * (gate * jax.nn.sigmoid(gate))).astype(
            BF16
        )
    out[...] = dot_t(mixin[...], w_out[...]).astype(BF16)
    for copy in copies:
        copy.wait()


def shaped(dims, dtype=BF16):
    return jax.ShapeDtypeStruct(dims, dtype)


def near(dims, dtype=BF16):
    return pltpu.VMEM(dims, dtype)


def held(value):
    return pltpu.with_memory_space_constraint(value, pltpu.VMEM)


def far(value):
    return pltpu.with_memory_space_constraint(value, pltpu.HBM)


def window_of(prefix_len, accepted, ctx_dev):
    offset = prefix_len[0] + accepted[0] - lax.axis_index("kv") * ctx_dev
    start = jnp.minimum(jnp.maximum(offset, 0), ctx_dev - WINDOW)
    return offset, pl.multiple_of((start >> 4) << 4, PROPS)


def local(
    tokens,
    norm_gain,
    w_query,
    w_key,
    w_value,
    w_gate,
    w_out,
    head_bias,
    cache_keys,
    cache_values,
    prefix_len,
    accepted,
    parent,
):
    inner_groups, outer_groups = groups_of(lax.axis_size("kv"))
    outer = len(outer_groups[0])
    columns, width = w_query.shape
    heads = width // HEAD
    rows = heads * PROPS
    share = -(-3 * heads // INNER) * PROPS
    sent = rows + share + PROPS
    keys = jnp.transpose(cache_keys[0], (1, 0, 2))
    values = jnp.transpose(cache_values[0], (1, 0, 2))

    pieces = pl.pallas_call(
        project_kernel,
        out_shape=near((INNER, sent, HEAD)),
        in_specs=[SMEM] * 2 + [ANY] * 6,
        out_specs=VMEM,
        scratch_shapes=[
            pltpu.VMEM(tokens.shape[1:], BF16),
            pltpu.VMEM((1, columns), F32),
            *[pltpu.VMEM(w_query.shape, BF16)] * 4,
            pltpu.SemaphoreType.DMA((6,)),
        ],
        name="project",
        compiler_params=PARAMS,
    )(
        prefix_len,
        accepted,
        *(
            far(value)
            for value in (tokens[0], norm_gain[None], w_query, w_key, w_value, w_gate)
        ),
    )
    pieces = pl.pallas_call(
        forward_kernel,
        out_shape=near((outer, sent, HEAD)),
        in_specs=[VMEM],
        out_specs=VMEM,
        name="forward",
        compiler_params=PARAMS,
    )(held(exchange(pieces, inner_groups)))
    window = near((heads, WINDOW, HEAD))
    pieces, query, keys_next, values_next, keys_window, values_window = pl.pallas_call(
        attend_kernel,
        out_shape=(
            near((INNER, sent, HEAD)),
            near((rows, HEAD)),
            shaped(keys.shape),
            shaped(values.shape),
            window,
            window,
        ),
        in_specs=[SMEM] * 3 + [VMEM] * 3,
        out_specs=(VMEM, VMEM, ANY, ANY, VMEM, VMEM),
        scratch_shapes=[pltpu.SemaphoreType.DMA((2,))],
        name="attend",
        compiler_params=PARAMS,
    )(
        prefix_len,
        accepted,
        head_bias,
        held(exchange(pieces, outer_groups)),
        held(keys),
        held(values),
    )
    pieces, fresh = pl.pallas_call(
        merge_kernel,
        out_shape=(near((outer, rows + PROPS, HEAD)), near((INNER * share, HEAD))),
        in_specs=[VMEM],
        out_specs=(VMEM, VMEM),
        name="merge",
        compiler_params=PARAMS,
    )(held(exchange(pieces, inner_groups)))
    part_out, keys_next, values_next = pl.pallas_call(
        finish_kernel,
        out_shape=(
            near((PROPS, w_out.shape[1])),
            shaped(keys.shape),
            shaped(values.shape),
        ),
        in_specs=[SMEM] * 4 + [VMEM] * 6 + [ANY, ANY],
        out_specs=(VMEM, ANY, ANY),
        input_output_aliases={10: 1, 11: 2},
        scratch_shapes=[
            pltpu.VMEM((PROPS, heads * HEAD), BF16),
            pltpu.VMEM((2, heads, WINDOW, HEAD), BF16),
            pltpu.SMEM((PROPS,), jnp.int32),
            pltpu.SemaphoreType.DMA((2,)),
        ],
        name="finish",
        compiler_params=PARAMS,
    )(
        prefix_len,
        accepted,
        head_bias,
        parent[0],
        held(exchange(pieces, outer_groups)),
        held(fresh),
        held(query),
        held(w_out.T),
        held(keys_window),
        held(values_window),
        keys_next,
        values_next,
    )
    both = lax.all_gather(part_out, "tp").astype(F32)
    mixed = both.sum(0).astype(BF16)[None]
    return (
        mixed,
        jnp.transpose(keys_next, (1, 0, 2))[None],
        jnp.transpose(values_next, (1, 0, 2))[None],
    )


def solution(mesh):
    return jax.shard_map(
        local,
        mesh=mesh,
        in_specs=(
            P("dp", None, "kv"),
            P("kv"),
            P("kv", "tp"),
            P("kv", "tp"),
            P("kv", "tp"),
            P("kv", "tp"),
            P("tp", "kv"),
            P("tp"),
            P("dp", "kv", "tp", None),
            P("dp", "kv", "tp", None),
            P("dp"),
            P("dp"),
            P("dp", None),
        ),
        out_specs=(P("dp", None, "kv"), P("dp", "kv", "tp", None), P("dp", "kv", "tp", None)),
        check_vma=False,
    )
```

```python
import jax
import jax.numpy as jnp
from jax import lax
from jax.experimental import pallas as pl
from jax.experimental.pallas import tpu as pltpu
from jax.sharding import PartitionSpec as P

D = 2048
HEAD = 128
EPS = 1e-06
INNER = 8
PROPS = 16
WINDOW = 32
STEPS = (2, 1, 3)
F32 = jnp.float32
BF16 = jnp.bfloat16
VMEM = pl.BlockSpec(memory_space=pltpu.VMEM)
SMEM = pl.BlockSpec(memory_space=pltpu.SMEM)
ANY = pl.BlockSpec(memory_space=pl.ANY)
PARAMS = pltpu.CompilerParams(vmem_limit_bytes=16 * 2**20)


def exchange(pieces):
    outer = lax.axis_size("kv") // INNER
    groups = [[a * INNER + i for i in range(INNER)] for a in range(outer)]
    return held(lax.all_to_all(pieces, "kv", 0, 0, axis_index_groups=groups, tiled=True))


def shifted(value):
    count = lax.axis_size("kv")
    parts = [value]
    for step in STEPS:
        pairs = [(spot, (spot + step * INNER) % count) for spot in range(count)]
        parts.append(lax.ppermute(value, "kv", pairs))
    return [held(part) for part in parts]


def iota(shape, dim):
    return lax.broadcasted_iota(jnp.int32, shape, dim)


def in_three(value):
    high = value.astype(BF16).astype(F32)
    rest = value - high
    middle = rest.astype(BF16).astype(F32)
    return high, middle, rest - middle


def dot(left, right):
    return jnp.dot(left, right, preferred_element_type=F32)


def dot_t(left, right):
    return lax.dot_general(left, right, (((1,), (1,)), ((), ())), preferred_element_type=F32)


def log_sigmoids(scores):
    soft = jnp.log1p(jnp.exp(-jnp.abs(scores)))
    return jnp.minimum(scores, 0.0) - soft, jnp.minimum(-scores, 0.0) - soft


def square_block(squares):
    lane = iota((PROPS, HEAD), 1)
    block = jnp.zeros((PROPS, HEAD), F32)
    for index, piece in enumerate(in_three(squares)):
        block = jnp.where(lane == index, piece, block)
    return block.astype(BF16)


def rest_block(rests):
    lane = iota((PROPS, HEAD), 1)
    block = jnp.zeros((PROPS, HEAD), F32)
    for index, rest in enumerate(rests):
        block = jnp.where(lane == index, rest, block)
    high, middle, low = in_three(block)
    block = high + pltpu.roll(middle, PROPS, 1) + pltpu.roll(low, 2 * PROPS, 1)
    return block.astype(BF16)


def rest_sums(block):
    block = block.astype(F32)
    return block + pltpu.roll(block, HEAD - PROPS, 1) + pltpu.roll(block, HEAD - 2 * PROPS, 1)


def after_table(width):
    row = iota((width, 2 * HEAD), 0)
    column = iota((width, 2 * HEAD), 1)
    return jnp.where((row > column) | (column >= HEAD), 1.0, 0.0).astype(BF16)


def after_and_all(values, table):
    high = values.astype(BF16)
    rest = values - high.astype(F32)
    middle = rest.astype(BF16)
    low = (rest - middle.astype(F32)).astype(BF16)
    sums = dot(high, table) + dot(middle, table) + dot(low, table)
    return sums[:, :HEAD], sums[:, HEAD:]


def project_kernel(
    prefix_len,
    accepted,
    tokens_far,
    gain_far,
    query_far,
    key_far,
    value_far,
    gate_far,
    out,
    tokens,
    gain,
    w_query,
    w_key,
    w_value,
    w_gate,
    sems,
):
    del prefix_len, accepted
    copies = [
        pltpu.make_async_copy(source, target, sems.at[index])
        for index, (source, target) in enumerate(
            (
                (tokens_far, tokens),
                (gain_far, gain),
                (query_far, w_query),
                (key_far, w_key),
                (value_far, w_value),
                (gate_far, w_gate),
            )
        )
    ]
    for copy in copies:
        copy.start()
    heads = w_query.shape[1] // HEAD
    rows = heads * PROPS
    share = out.shape[1] - rows - PROPS
    copies[0].wait()
    flat = tokens[...].astype(F32)
    block = square_block(jnp.sum(flat * flat, axis=1, keepdims=True))
    copies[1].wait()
    scaled = (flat * gain[...]).astype(BF16)
    copies[2].wait()
    query = dot(scaled, w_query[...]).astype(BF16)
    for dest in range(INNER):
        for head in range(heads):
            out[dest, head * PROPS : (head + 1) * PROPS, :] = query[
                :, head * HEAD : (head + 1) * HEAD
            ]
        out[dest, rows + share :, :] = block
    slots = share // PROPS
    for which, weight in enumerate((w_key, w_value, w_gate)):
        copies[3 + which].wait()
        part = dot(scaled, weight[...]).astype(BF16)
        for head in range(heads):
            dest, slot = divmod(which * heads + head, slots)
            out[dest, rows + slot * PROPS : rows + (slot + 1) * PROPS, :] = part[
                :, head * HEAD : (head + 1) * HEAD
            ]
    for spare in range(3 * heads, INNER * slots):
        dest, slot = divmod(spare, slots)
        out[dest, rows + slot * PROPS : rows + (slot + 1) * PROPS, :] = jnp.zeros(
            (PROPS, HEAD), BF16
        )


def add_up(parts):
    total = parts[0].astype(F32)
    for part in parts[1:]:
        total = total + part.astype(F32)
    return total


def forward_kernel(arrived, out):
    count = arrived.shape[1] - PROPS
    total = add_up([arrived[source] for source in range(INNER)])
    out[:count, :] = total[:count].astype(BF16)
    out[count:, :] = square_block(jnp.sum(total[count:], axis=1, keepdims=True))


def attend_kernel(
    prefix_len,
    accepted,
    bias,
    own,
    first_part,
    second_part,
    third_part,
    keys,
    values,
    out,
    query_out,
    keys_next,
    values_next,
    keys_window,
    values_window,
    sems,
):
    heads, ctx_dev, _ = keys.shape
    rows = heads * PROPS
    copies = [
        pltpu.make_async_copy(keys, keys_next, sems.at[0]),
        pltpu.make_async_copy(values, values_next, sems.at[1]),
    ]
    for copy in copies:
        copy.start()
    offset, first = window_of(prefix_len, accepted, ctx_dev)
    total = add_up([own[...], first_part[...], second_part[...], third_part[...]])
    squares = jnp.sum(total[own.shape[0] - PROPS :], axis=1, keepdims=True)
    rscale = lax.rsqrt(squares / D + EPS)
    share = own.shape[0] - PROPS - rows
    for slot in range(share // PROPS):
        there = slice(rows + slot * PROPS, rows + (slot + 1) * PROPS)
        piece = (total[there] * rscale).astype(BF16)
        for dest in range(INNER):
            out[dest, there, :] = piece
    factor = HEAD ** (-0.5)
    live = iota((PROPS, ctx_dev), 1) < offset
    takes, keeps = [], []
    for head in range(heads):
        there = slice(head * PROPS, (head + 1) * PROPS)
        query = (total[there] * rscale).astype(BF16)
        query_out[there, :] = query
        scores = dot_t(query, keys[head]) * factor + bias[head]
        take, keep = log_sigmoids(scores)
        takes.append(take)
        keeps.append(jnp.where(live, keep, 0.0))
    keep = jnp.concatenate(keeps, axis=0)
    table = after_table(HEAD)
    beyond = jnp.zeros((rows, HEAD), F32)
    laters = []
    for chunk in reversed(range(ctx_dev // HEAD)):
        inside, whole = after_and_all(keep[:, chunk * HEAD : (chunk + 1) * HEAD], table)
        laters.append(inside + beyond)
        beyond = beyond + whole
    later = jnp.concatenate(laters[::-1], axis=1)
    rests = []
    for head in range(heads):
        there = slice(head * PROPS, (head + 1) * PROPS)
        weight = jnp.where(live, jnp.exp(takes[head] + later[there]), 0.0).astype(BF16)
        summed = dot(weight, values[head]).astype(BF16)
        for dest in range(INNER):
            out[dest, there, :] = summed
        rests.append(beyond[there])
    block = rest_block(rests)
    for dest in range(INNER):
        out[dest, rows + share :, :] = block
    keys_window[...] = keys[:, pl.ds(first, WINDOW), :]
    values_window[...] = values[:, pl.ds(first, WINDOW), :]
    for copy in copies:
        copy.wait()


def merge_kernel(arrived, out, fresh):
    count = arrived.shape[0]
    rows = out.shape[0] - PROPS
    heads = rows // PROPS
    share = arrived.shape[1] - PROPS - rows
    for source in range(count):
        fresh[source * share : (source + 1) * share, :] = arrived[source, rows : rows + share, :]
    beyond = jnp.zeros((PROPS, HEAD), F32)
    factors = []
    for source in reversed(range(count)):
        factors.append(jnp.exp(beyond))
        beyond = beyond + rest_sums(arrived[source, rows + share :, :])
    factors = factors[::-1]
    for head in range(heads):
        there = slice(head * PROPS, (head + 1) * PROPS)
        total = jnp.zeros((PROPS, HEAD), F32)
        for source in range(count):
            total = total + factors[source][:, head : head + 1] * arrived[
                source, there, :
            ].astype(F32)
        out[there, :] = total.astype(BF16)
    out[rows:, :] = rest_block([beyond[:, head : head + 1] for head in range(heads)])


def tree_kernel(
    prefix_len,
    accepted,
    bias,
    parent,
    fresh,
    query,
    keys_window,
    values_window,
    keys_old,
    values_old,
    tree_out,
    tail_out,
    gate_out,
    keys_next,
    values_next,
    patches,
    masks,
    sems,
):
    del keys_old, values_old
    heads, ctx_dev, _ = keys_next.shape
    offset, first = window_of(prefix_len, accepted, ctx_dev)
    source = first + iota((WINDOW, PROPS), 0) - offset
    picker = jnp.where(source == iota((WINDOW, PROPS), 1), 1.0, 0.0).astype(BF16)
    source = first + iota((WINDOW, HEAD), 0) - offset
    inside = (source >= 0) & (source < PROPS)
    copies = []
    for which, (window, target) in enumerate(
        ((keys_window, keys_next), (values_window, values_next))
    ):
        for head in range(heads):
            start = (which * heads + head) * PROPS
            placed = dot(picker, fresh[start : start + PROPS, :])
            patches[which, head] = jnp.where(inside, placed, window[head].astype(F32)).astype(BF16)
        copies.append(
            pltpu.make_async_copy(
                patches.at[which], target.at[:, pl.ds(first, WINDOW), :], sems.at[which]
            )
        )
        copies[-1].start()
    row = iota((PROPS, PROPS), 0)
    reach = jnp.zeros((PROPS, PROPS), jnp.int32)
    masks[0] = 0
    for index in range(1, PROPS):
        above = parent[index]
        mask = masks[above] | (1 << above)
        masks[index] = mask
        reach = jnp.where(row == index, mask, reach)
    family = ((reach >> iota((PROPS, PROPS), 1)) & 1) == 1
    factor = HEAD ** (-0.5)
    takes, keeps = [], []
    for head in range(heads):
        there = slice(head * PROPS, (head + 1) * PROPS)
        scores = dot_t(query[there, :], fresh[there, :]) * factor + bias[head]
        take, keep = log_sigmoids(scores)
        takes.append(take)
        keeps.append(jnp.where(family, keep, 0.0))
    later, tail = after_and_all(jnp.concatenate(keeps, axis=0), after_table(PROPS))
    tail_out[...] = tail
    for head in range(heads):
        there = slice(head * PROPS, (head + 1) * PROPS)
        weight = jnp.where(family, jnp.exp(takes[head] + later[there, :PROPS]), 0.0).astype(BF16)
        start = (heads + head) * PROPS
        tree_out[there, :] = dot(weight, fresh[start : start + PROPS, :])
    gate = fresh[2 * heads * PROPS : 3 * heads * PROPS, :].astype(F32)
    gate_out[...] = gate * jax.nn.sigmoid(gate)
    for copy in copies:
        copy.wait()


def finish_kernel(tree, tail, gate, w_out, own, first_part, second_part, third_part, out, mixin):
    parts = (own, first_part, second_part, third_part)
    outer = len(parts)
    rows = own.shape[0] - PROPS
    heads = rows // PROPS
    place = lax.axis_index("kv") // INNER
    spots = [lax.rem(place + outer - step, outer) for step in (0, *STEPS)]
    rests = [rest_sums(part[rows:, :]) for part in parts]
    beyonds = []
    for spot in spots:
        beyond = jnp.zeros((PROPS, HEAD), F32)
        for other, rest in zip(spots, rests):
            beyond = beyond + jnp.where(other > spot, rest, 0.0)
        beyonds.append(beyond)
    for head in range(heads):
        there = slice(head * PROPS, (head + 1) * PROPS)
        total = tree[there, :]
        for part, beyond in zip(parts, beyonds):
            total = total + jnp.exp(beyond[:, head : head + 1] + tail[there, :]) * part[
                there, :
            ].astype(F32)
        mixin[:, head * HEAD : (head + 1) * HEAD] = (total * gate[there, :]).astype(BF16)
    out[...] = dot_t(mixin[...], w_out[...]).astype(BF16)


def shaped(dims, dtype=BF16):
    return jax.ShapeDtypeStruct(dims, dtype)


def near(dims, dtype=BF16):
    return pltpu.VMEM(dims, dtype)


def held(value):
    return pltpu.with_memory_space_constraint(value, pltpu.VMEM)


def far(value):
    return pltpu.with_memory_space_constraint(value, pltpu.HBM)


def window_of(prefix_len, accepted, ctx_dev):
    offset = prefix_len[0] + accepted[0] - lax.axis_index("kv") * ctx_dev
    start = jnp.minimum(jnp.maximum(offset, 0), ctx_dev - WINDOW)
    return offset, pl.multiple_of((start >> 4) << 4, PROPS)


def local(
    tokens,
    norm_gain,
    w_query,
    w_key,
    w_value,
    w_gate,
    w_out,
    head_bias,
    cache_keys,
    cache_values,
    prefix_len,
    accepted,
    parent,
):
    columns, width = w_query.shape
    heads = width // HEAD
    rows = heads * PROPS
    share = -(-3 * heads // INNER) * PROPS
    sent = rows + share + PROPS
    keys = jnp.transpose(cache_keys[0], (1, 0, 2))
    values = jnp.transpose(cache_values[0], (1, 0, 2))

    pieces = pl.pallas_call(
        project_kernel,
        out_shape=near((INNER, sent, HEAD)),
        in_specs=[SMEM] * 2 + [ANY] * 6,
        out_specs=VMEM,
        scratch_shapes=[
            pltpu.VMEM(tokens.shape[1:], BF16),
            pltpu.VMEM((1, columns), F32),
            *[pltpu.VMEM(w_query.shape, BF16)] * 4,
            pltpu.SemaphoreType.DMA((6,)),
        ],
        name="project",
        compiler_params=PARAMS,
    )(
        prefix_len,
        accepted,
        *(
            far(value)
            for value in (tokens[0], norm_gain[None], w_query, w_key, w_value, w_gate)
        ),
    )
    pieces = pl.pallas_call(
        forward_kernel,
        out_shape=near((sent, HEAD)),
        in_specs=[VMEM],
        out_specs=VMEM,
        name="forward",
        compiler_params=PARAMS,
    )(exchange(pieces))
    window = near((heads, WINDOW, HEAD))
    pieces, query, keys_next, values_next, keys_window, values_window = pl.pallas_call(
        attend_kernel,
        out_shape=(
            near((INNER, sent, HEAD)),
            near((rows, HEAD)),
            shaped(keys.shape),
            shaped(values.shape),
            window,
            window,
        ),
        in_specs=[SMEM] * 3 + [VMEM] * 6,
        out_specs=(VMEM, VMEM, ANY, ANY, VMEM, VMEM),
        scratch_shapes=[pltpu.SemaphoreType.DMA((2,))],
        name="attend",
        compiler_params=PARAMS,
    )(
        prefix_len,
        accepted,
        head_bias,
        *shifted(pieces),
        held(keys),
        held(values),
    )
    pieces, fresh = pl.pallas_call(
        merge_kernel,
        out_shape=(near((rows + PROPS, HEAD)), near((INNER * share, HEAD))),
        in_specs=[VMEM],
        out_specs=(VMEM, VMEM),
        name="merge",
        compiler_params=PARAMS,
    )(exchange(pieces))
    parts = shifted(pieces)
    tree, tail, gate, keys_next, values_next = pl.pallas_call(
        tree_kernel,
        out_shape=(
            *[near((rows, HEAD), F32)] * 3,
            shaped(keys.shape),
            shaped(values.shape),
        ),
        in_specs=[SMEM] * 4 + [VMEM] * 4 + [ANY, ANY],
        out_specs=(VMEM, VMEM, VMEM, ANY, ANY),
        input_output_aliases={8: 3, 9: 4},
        scratch_shapes=[
            pltpu.VMEM((2, heads, WINDOW, HEAD), BF16),
            pltpu.SMEM((PROPS,), jnp.int32),
            pltpu.SemaphoreType.DMA((2,)),
        ],
        name="tree",
        compiler_params=PARAMS,
    )(
        prefix_len,
        accepted,
        head_bias,
        parent[0],
        held(fresh),
        held(query),
        held(keys_window),
        held(values_window),
        keys_next,
        values_next,
    )
    part_out = pl.pallas_call(
        finish_kernel,
        out_shape=near((PROPS, w_out.shape[1])),
        in_specs=[VMEM] * 8,
        out_specs=VMEM,
        scratch_shapes=[pltpu.VMEM((PROPS, heads * HEAD), BF16)],
        name="finish",
        compiler_params=PARAMS,
    )(held(tree), held(tail), held(gate), held(w_out.T), *parts)
    other = lax.ppermute(part_out, "tp", [(0, 1), (1, 0)])
    mixed = (part_out.astype(F32) + other.astype(F32)).astype(BF16)[None]
    return (
        mixed,
        jnp.transpose(keys_next, (1, 0, 2))[None],
        jnp.transpose(values_next, (1, 0, 2))[None],
    )


def solution(mesh):
    return jax.shard_map(
        local,
        mesh=mesh,
        in_specs=(
            P("dp", None, "kv"),
            P("kv"),
            P("kv", "tp"),
            P("kv", "tp"),
            P("kv", "tp"),
            P("kv", "tp"),
            P("tp", "kv"),
            P("tp"),
            P("dp", "kv", "tp", None),
            P("dp", "kv", "tp", None),
            P("dp"),
            P("dp"),
            P("dp", None),
        ),
        out_specs=(P("dp", None, "kv"), P("dp", "kv", "tp", None), P("dp", "kv", "tp", None)),
        check_vma=False,
    )
```

```python
import jax
import jax.numpy as jnp
from jax import lax
from jax.experimental import pallas as pl
from jax.experimental.pallas import tpu as pltpu
from jax.sharding import PartitionSpec as P

D = 2048
HEAD = 128
EPS = 1e-06
INNER = 8
PROPS = 16
WINDOW = 32
STEPS = (2, 1, 3)
F32 = jnp.float32
BF16 = jnp.bfloat16
VMEM = pl.BlockSpec(memory_space=pltpu.VMEM)
SMEM = pl.BlockSpec(memory_space=pltpu.SMEM)
ANY = pl.BlockSpec(memory_space=pl.ANY)
PARAMS = pltpu.CompilerParams(vmem_limit_bytes=16 * 2**20)


def exchange(pieces):
    outer = lax.axis_size("kv") // INNER
    groups = [[a * INNER + i for i in range(INNER)] for a in range(outer)]
    return held(lax.all_to_all(pieces, "kv", 0, 0, axis_index_groups=groups, tiled=True))


def shifted(value):
    count = lax.axis_size("kv")
    parts = [value]
    for step in STEPS:
        pairs = [(spot, (spot + step * INNER) % count) for spot in range(count)]
        parts.append(lax.ppermute(value, "kv", pairs))
    return [held(part) for part in parts]


def iota(shape, dim):
    return lax.broadcasted_iota(jnp.int32, shape, dim)


def in_three(value):
    high = value.astype(BF16).astype(F32)
    rest = value - high
    middle = rest.astype(BF16).astype(F32)
    return high, middle, rest - middle


def dot(left, right):
    return jnp.dot(left, right, preferred_element_type=F32)


def dot_t(left, right):
    return lax.dot_general(left, right, (((1,), (1,)), ((), ())), preferred_element_type=F32)


def log_sigmoids(scores):
    soft = jnp.log1p(jnp.exp(-jnp.abs(scores)))
    return jnp.minimum(scores, 0.0) - soft, jnp.minimum(-scores, 0.0) - soft


def square_block(squares):
    lane = iota((PROPS, HEAD), 1)
    block = jnp.zeros((PROPS, HEAD), F32)
    for index, piece in enumerate(in_three(squares)):
        block = jnp.where(lane == index, piece, block)
    return block.astype(BF16)


def rest_block(rests):
    lane = iota((PROPS, HEAD), 1)
    block = jnp.zeros((PROPS, HEAD), F32)
    for index, rest in enumerate(rests):
        block = jnp.where(lane == index, rest, block)
    high, middle, low = in_three(block)
    block = high + pltpu.roll(middle, PROPS, 1) + pltpu.roll(low, 2 * PROPS, 1)
    return block.astype(BF16)


def rest_sums(block):
    block = block.astype(F32)
    return block + pltpu.roll(block, HEAD - PROPS, 1) + pltpu.roll(block, HEAD - 2 * PROPS, 1)


def after_table(width):
    row = iota((width, 2 * HEAD), 0)
    column = iota((width, 2 * HEAD), 1)
    return jnp.where((row > column) | (column >= HEAD), 1.0, 0.0).astype(BF16)


def after_and_all(values, table):
    high = values.astype(BF16)
    rest = values - high.astype(F32)
    middle = rest.astype(BF16)
    low = (rest - middle.astype(F32)).astype(BF16)
    sums = dot(high, table) + dot(middle, table) + dot(low, table)
    return sums[:, :HEAD], sums[:, HEAD:]


def project_kernel(
    bias_far,
    parent_far,
    tokens_far,
    gain_far,
    query_far,
    key_far,
    value_far,
    gate_far,
    out,
    bias,
    parent,
    tokens,
    gain,
    w_query,
    w_key,
    w_value,
    w_gate,
    sems,
):
    copies = [
        pltpu.make_async_copy(source, target, sems.at[index])
        for index, (source, target) in enumerate(
            (
                (tokens_far, tokens),
                (gain_far, gain),
                (query_far, w_query),
                (key_far, w_key),
                (value_far, w_value),
                (gate_far, w_gate),
                (bias_far, bias),
                (parent_far, parent),
            )
        )
    ]
    for copy in copies:
        copy.start()
    heads = w_query.shape[1] // HEAD
    rows = heads * PROPS
    share = out.shape[1] - rows - PROPS
    copies[0].wait()
    flat = tokens[...].astype(F32)
    block = square_block(jnp.sum(flat * flat, axis=1, keepdims=True))
    copies[1].wait()
    scaled = (flat * gain[...]).astype(BF16)
    copies[2].wait()
    query = dot(scaled, w_query[...]).astype(BF16)
    for dest in range(INNER):
        for head in range(heads):
            out[dest, head * PROPS : (head + 1) * PROPS, :] = query[
                :, head * HEAD : (head + 1) * HEAD
            ]
        out[dest, rows + share :, :] = block
    slots = share // PROPS
    for which, weight in enumerate((w_key, w_value, w_gate)):
        copies[3 + which].wait()
        part = dot(scaled, weight[...]).astype(BF16)
        for head in range(heads):
            dest, slot = divmod(which * heads + head, slots)
            out[dest, rows + slot * PROPS : rows + (slot + 1) * PROPS, :] = part[
                :, head * HEAD : (head + 1) * HEAD
            ]
    for spare in range(3 * heads, INNER * slots):
        dest, slot = divmod(spare, slots)
        out[dest, rows + slot * PROPS : rows + (slot + 1) * PROPS, :] = jnp.zeros(
            (PROPS, HEAD), BF16
        )
    for copy in copies[6:]:
        copy.wait()


def add_up(parts):
    total = parts[0].astype(F32)
    for part in parts[1:]:
        total = total + part.astype(F32)
    return total


def forward_kernel(arrived, out):
    count = arrived.shape[1] - PROPS
    total = add_up([arrived[source] for source in range(INNER)])
    out[:count, :] = total[:count].astype(BF16)
    out[count:, :] = square_block(jnp.sum(total[count:], axis=1, keepdims=True))


def attend_kernel(
    prefix_len,
    accepted,
    bias,
    own,
    first_part,
    second_part,
    third_part,
    keys,
    values_far,
    out,
    query_out,
    values,
    limits,
    sem,
):
    heads, ctx_dev, _ = keys.shape
    rows = heads * PROPS
    load = pltpu.make_async_copy(values_far, values, sem)
    load.start()
    offset = prefix_len[0] + accepted[0] - lax.axis_index("kv") * ctx_dev
    first = jnp.minimum(jnp.maximum(offset, 0), ctx_dev - WINDOW)
    first = pl.multiple_of((first >> 4) << 4, PROPS)
    limits[0] = offset
    limits[1] = first
    total = add_up([own[...], first_part[...], second_part[...], third_part[...]])
    squares = jnp.sum(total[own.shape[0] - PROPS :], axis=1, keepdims=True)
    rscale = lax.rsqrt(squares / D + EPS)
    share = own.shape[0] - PROPS - rows
    for slot in range(share // PROPS):
        there = slice(rows + slot * PROPS, rows + (slot + 1) * PROPS)
        piece = (total[there] * rscale).astype(BF16)
        for dest in range(INNER):
            out[dest, there, :] = piece
    factor = HEAD ** (-0.5)
    live = iota((PROPS, ctx_dev), 1) < offset
    takes, keeps = [], []
    for head in range(heads):
        there = slice(head * PROPS, (head + 1) * PROPS)
        query = (total[there] * rscale).astype(BF16)
        query_out[there, :] = query
        scores = dot_t(query, keys[head]) * factor + bias[head]
        take, keep = log_sigmoids(scores)
        takes.append(take)
        keeps.append(jnp.where(live, keep, 0.0))
    keep = jnp.concatenate(keeps, axis=0)
    table = after_table(HEAD)
    beyond = jnp.zeros((rows, HEAD), F32)
    laters = []
    for chunk in reversed(range(ctx_dev // HEAD)):
        inside, whole = after_and_all(keep[:, chunk * HEAD : (chunk + 1) * HEAD], table)
        laters.append(inside + beyond)
        beyond = beyond + whole
    later = jnp.concatenate(laters[::-1], axis=1)
    load.wait()
    rests = []
    for head in range(heads):
        there = slice(head * PROPS, (head + 1) * PROPS)
        weight = jnp.where(live, jnp.exp(takes[head] + later[there]), 0.0).astype(BF16)
        summed = dot(weight, values[head]).astype(BF16)
        for dest in range(INNER):
            out[dest, there, :] = summed
        rests.append(beyond[there])
    block = rest_block(rests)
    for dest in range(INNER):
        out[dest, rows + share :, :] = block


def merge_kernel(arrived, out, fresh):
    count = arrived.shape[0]
    rows = out.shape[0] - PROPS
    heads = rows // PROPS
    share = arrived.shape[1] - PROPS - rows
    for source in range(count):
        fresh[source * share : (source + 1) * share, :] = arrived[source, rows : rows + share, :]
    beyond = jnp.zeros((PROPS, HEAD), F32)
    factors = []
    for source in reversed(range(count)):
        factors.append(jnp.exp(beyond))
        beyond = beyond + rest_sums(arrived[source, rows + share :, :])
    factors = factors[::-1]
    for head in range(heads):
        there = slice(head * PROPS, (head + 1) * PROPS)
        total = jnp.zeros((PROPS, HEAD), F32)
        for source in range(count):
            total = total + factors[source][:, head : head + 1] * arrived[
                source, there, :
            ].astype(F32)
        out[there, :] = total.astype(BF16)
    out[rows:, :] = rest_block([beyond[:, head : head + 1] for head in range(heads)])


def tree_kernel(
    limits,
    bias,
    parent,
    fresh,
    query,
    keys,
    values,
    tree_out,
    tail_out,
    gate_out,
    keys_next,
    values_next,
    patches,
    masks,
    sems,
):
    heads = keys_next.shape[0]
    bulk = [
        pltpu.make_async_copy(keys, keys_next, sems.at[0]),
        pltpu.make_async_copy(values, values_next, sems.at[1]),
    ]
    for copy in bulk:
        copy.start()
    offset = limits[0]
    first = pl.multiple_of(limits[1], PROPS)
    source = first + iota((WINDOW, PROPS), 0) - offset
    picker = jnp.where(source == iota((WINDOW, PROPS), 1), 1.0, 0.0).astype(BF16)
    source = first + iota((WINDOW, HEAD), 0) - offset
    inside = (source >= 0) & (source < PROPS)
    copies = []
    for which, (cache, target) in enumerate(((keys, keys_next), (values, values_next))):
        for head in range(heads):
            start = (which * heads + head) * PROPS
            placed = dot(picker, fresh[start : start + PROPS, :])
            there = cache[head, pl.ds(first, WINDOW), :].astype(F32)
            patches[which, head] = jnp.where(inside, placed, there).astype(BF16)
        copies.append(
            pltpu.make_async_copy(
                patches.at[which], target.at[:, pl.ds(first, WINDOW), :], sems.at[2 + which]
            )
        )
    row = iota((PROPS, PROPS), 0)
    reach = jnp.zeros((PROPS, PROPS), jnp.int32)
    masks[0] = 0
    for index in range(1, PROPS):
        above = parent[index]
        mask = masks[above] | (1 << above)
        masks[index] = mask
        reach = jnp.where(row == index, mask, reach)
    family = ((reach >> iota((PROPS, PROPS), 1)) & 1) == 1
    factor = HEAD ** (-0.5)
    takes, keeps = [], []
    for head in range(heads):
        there = slice(head * PROPS, (head + 1) * PROPS)
        scores = dot_t(query[there, :], fresh[there, :]) * factor + bias[head]
        take, keep = log_sigmoids(scores)
        takes.append(take)
        keeps.append(jnp.where(family, keep, 0.0))
    later, tail = after_and_all(jnp.concatenate(keeps, axis=0), after_table(PROPS))
    tail_out[...] = tail
    for head in range(heads):
        there = slice(head * PROPS, (head + 1) * PROPS)
        weight = jnp.where(family, jnp.exp(takes[head] + later[there, :PROPS]), 0.0).astype(BF16)
        start = (heads + head) * PROPS
        tree_out[there, :] = dot(weight, fresh[start : start + PROPS, :])
    gate = fresh[2 * heads * PROPS : 3 * heads * PROPS, :].astype(F32)
    gate_out[...] = gate * jax.nn.sigmoid(gate)
    for before, copy in zip(bulk, copies):
        before.wait()
        copy.start()
    for copy in copies:
        copy.wait()


def finish_kernel(tree, tail, gate, w_out, own, first_part, second_part, third_part, out, mixin):
    parts = (own, first_part, second_part, third_part)
    outer = len(parts)
    rows = own.shape[0] - PROPS
    heads = rows // PROPS
    place = lax.axis_index("kv") // INNER
    spots = [lax.rem(place + outer - step, outer) for step in (0, *STEPS)]
    rests = [rest_sums(part[rows:, :]) for part in parts]
    beyonds = []
    for spot in spots:
        beyond = jnp.zeros((PROPS, HEAD), F32)
        for other, rest in zip(spots, rests):
            beyond = beyond + jnp.where(other > spot, rest, 0.0)
        beyonds.append(beyond)
    for head in range(heads):
        there = slice(head * PROPS, (head + 1) * PROPS)
        total = tree[there, :]
        for part, beyond in zip(parts, beyonds):
            total = total + jnp.exp(beyond[:, head : head + 1] + tail[there, :]) * part[
                there, :
            ].astype(F32)
        mixin[:, head * HEAD : (head + 1) * HEAD] = (total * gate[there, :]).astype(BF16)
    out[...] = dot_t(mixin[...], w_out[...]).astype(BF16)


def shaped(dims, dtype=BF16):
    return jax.ShapeDtypeStruct(dims, dtype)


def near(dims, dtype=BF16):
    return pltpu.VMEM(dims, dtype)


def held(value):
    return pltpu.with_memory_space_constraint(value, pltpu.VMEM)


def small(dims, dtype):
    return pltpu.SMEM(dims, dtype)


def far(value):
    return pltpu.with_memory_space_constraint(value, pltpu.HBM)


def kept(value):
    return pltpu.with_memory_space_constraint(value, pltpu.SMEM)


def local(
    tokens,
    norm_gain,
    w_query,
    w_key,
    w_value,
    w_gate,
    w_out,
    head_bias,
    cache_keys,
    cache_values,
    prefix_len,
    accepted,
    parent,
):
    columns, width = w_query.shape
    heads = width // HEAD
    rows = heads * PROPS
    share = -(-3 * heads // INNER) * PROPS
    sent = rows + share + PROPS
    keys = jnp.transpose(cache_keys[0], (1, 0, 2))
    values = jnp.transpose(cache_values[0], (1, 0, 2))

    pieces, bias, parents = pl.pallas_call(
        project_kernel,
        out_shape=(
            near((INNER, sent, HEAD)),
            small((heads,), F32),
            small((PROPS,), jnp.int32),
        ),
        in_specs=[ANY] * 8,
        out_specs=(VMEM, SMEM, SMEM),
        scratch_shapes=[
            pltpu.VMEM(tokens.shape[1:], BF16),
            pltpu.VMEM((1, columns), F32),
            *[pltpu.VMEM(w_query.shape, BF16)] * 4,
            pltpu.SemaphoreType.DMA((8,)),
        ],
        name="project",
        compiler_params=PARAMS,
    )(
        *(
            far(value)
            for value in (
                head_bias,
                parent[0],
                tokens[0],
                norm_gain[None],
                w_query,
                w_key,
                w_value,
                w_gate,
            )
        ),
    )
    bias, parents = kept(bias), kept(parents)
    pieces = pl.pallas_call(
        forward_kernel,
        out_shape=near((sent, HEAD)),
        in_specs=[VMEM],
        out_specs=VMEM,
        name="forward",
        compiler_params=PARAMS,
    )(exchange(pieces))
    keys = held(keys)
    pieces, query, near_values, limits = pl.pallas_call(
        attend_kernel,
        out_shape=(
            near((INNER, sent, HEAD)),
            near((rows, HEAD)),
            near(values.shape),
            small((2,), jnp.int32),
        ),
        in_specs=[SMEM] * 3 + [VMEM] * 5 + [ANY],
        out_specs=(VMEM, VMEM, VMEM, SMEM),
        scratch_shapes=[pltpu.SemaphoreType.DMA],
        name="attend",
        compiler_params=PARAMS,
    )(
        prefix_len,
        accepted,
        bias,
        *shifted(pieces),
        keys,
        far(values),
    )
    pieces, fresh = pl.pallas_call(
        merge_kernel,
        out_shape=(near((rows + PROPS, HEAD)), near((INNER * share, HEAD))),
        in_specs=[VMEM],
        out_specs=(VMEM, VMEM),
        name="merge",
        compiler_params=PARAMS,
    )(exchange(pieces))
    parts = shifted(pieces)
    tree, tail, gate, keys_next, values_next = pl.pallas_call(
        tree_kernel,
        out_shape=(
            *[near((rows, HEAD), F32)] * 3,
            shaped(keys.shape),
            shaped(values.shape),
        ),
        in_specs=[SMEM] * 3 + [VMEM] * 4,
        out_specs=(VMEM, VMEM, VMEM, ANY, ANY),
        scratch_shapes=[
            pltpu.VMEM((2, heads, WINDOW, HEAD), BF16),
            pltpu.SMEM((PROPS,), jnp.int32),
            pltpu.SemaphoreType.DMA((4,)),
        ],
        name="tree",
        compiler_params=PARAMS,
    )(
        kept(limits),
        bias,
        parents,
        held(fresh),
        held(query),
        keys,
        held(near_values),
    )
    part_out = pl.pallas_call(
        finish_kernel,
        out_shape=near((PROPS, w_out.shape[1])),
        in_specs=[VMEM] * 8,
        out_specs=VMEM,
        scratch_shapes=[pltpu.VMEM((PROPS, heads * HEAD), BF16)],
        name="finish",
        compiler_params=PARAMS,
    )(held(tree), held(tail), held(gate), held(w_out.T), *parts)
    other = lax.ppermute(part_out, "tp", [(0, 1), (1, 0)])
    mixed = (part_out.astype(F32) + other.astype(F32)).astype(BF16)[None]
    return (
        mixed,
        jnp.transpose(keys_next, (1, 0, 2))[None],
        jnp.transpose(values_next, (1, 0, 2))[None],
    )


def solution(mesh):
    return jax.shard_map(
        local,
        mesh=mesh,
        in_specs=(
            P("dp", None, "kv"),
            P("kv"),
            P("kv", "tp"),
            P("kv", "tp"),
            P("kv", "tp"),
            P("kv", "tp"),
            P("tp", "kv"),
            P("tp"),
            P("dp", "kv", "tp", None),
            P("dp", "kv", "tp", None),
            P("dp"),
            P("dp"),
            P("dp", None),
        ),
        out_specs=(P("dp", None, "kv"), P("dp", "kv", "tp", None), P("dp", "kv", "tp", None)),
        check_vma=False,
    )
```

```python
import jax
import jax.numpy as jnp
from jax import lax
from jax.experimental import pallas as pl
from jax.experimental.pallas import tpu as pltpu
from jax.sharding import PartitionSpec as P

D = 2048
HEAD = 128
EPS = 1e-06
INNER = 8
PROPS = 16
WINDOW = 32
STEPS = (2, 1, 3)
F32 = jnp.float32
BF16 = jnp.bfloat16
VMEM = pl.BlockSpec(memory_space=pltpu.VMEM)
SMEM = pl.BlockSpec(memory_space=pltpu.SMEM)
ANY = pl.BlockSpec(memory_space=pl.ANY)
PARAMS = pltpu.CompilerParams(vmem_limit_bytes=16 * 2**20)


def exchange(pieces):
    outer = lax.axis_size("kv") // INNER
    groups = [[a * INNER + i for i in range(INNER)] for a in range(outer)]
    return held(lax.all_to_all(pieces, "kv", 0, 0, axis_index_groups=groups, tiled=True))


def shifted(value):
    count = lax.axis_size("kv")
    parts = [value]
    for step in STEPS:
        pairs = [(spot, (spot + step * INNER) % count) for spot in range(count)]
        parts.append(lax.ppermute(value, "kv", pairs))
    return [held(part) for part in parts]


def iota(shape, dim):
    return lax.broadcasted_iota(jnp.int32, shape, dim)


def in_three(value):
    high = value.astype(BF16).astype(F32)
    rest = value - high
    middle = rest.astype(BF16).astype(F32)
    return high, middle, rest - middle


def dot(left, right):
    return jnp.dot(left, right, preferred_element_type=F32)


def dot_t(left, right):
    return lax.dot_general(left, right, (((1,), (1,)), ((), ())), preferred_element_type=F32)


def log_sigmoids(scores):
    soft = jnp.log1p(jnp.exp(-jnp.abs(scores)))
    return jnp.minimum(scores, 0.0) - soft, jnp.minimum(-scores, 0.0) - soft


def square_block(squares):
    lane = iota((PROPS, HEAD), 1)
    block = jnp.zeros((PROPS, HEAD), F32)
    for index, piece in enumerate(in_three(squares)):
        block = jnp.where(lane == index, piece, block)
    return block.astype(BF16)


def rest_block(rests):
    lane = iota((PROPS, HEAD), 1)
    block = jnp.zeros((PROPS, HEAD), F32)
    for index, rest in enumerate(rests):
        block = jnp.where(lane == index, rest, block)
    high, middle, low = in_three(block)
    block = high + pltpu.roll(middle, PROPS, 1) + pltpu.roll(low, 2 * PROPS, 1)
    return block.astype(BF16)


def rest_sums(block):
    block = block.astype(F32)
    return block + pltpu.roll(block, HEAD - PROPS, 1) + pltpu.roll(block, HEAD - 2 * PROPS, 1)


def after_table(width):
    row = iota((width, 2 * HEAD), 0)
    column = iota((width, 2 * HEAD), 1)
    return jnp.where((row > column) | (column >= HEAD), 1.0, 0.0).astype(BF16)


def after_and_all(values, table):
    high = values.astype(BF16)
    rest = values - high.astype(F32)
    middle = rest.astype(BF16)
    low = (rest - middle.astype(F32)).astype(BF16)
    sums = dot(high, table) + dot(middle, table) + dot(low, table)
    return sums[:, :HEAD], sums[:, HEAD:]


def project_kernel(
    bias_far,
    parent_far,
    tokens_far,
    gain_far,
    query_far,
    key_far,
    value_far,
    gate_far,
    out,
    bias,
    parent,
    tokens,
    gain,
    w_query,
    w_key,
    w_value,
    w_gate,
    sems,
):
    copies = [
        pltpu.make_async_copy(source, target, sems.at[index])
        for index, (source, target) in enumerate(
            (
                (tokens_far, tokens),
                (gain_far, gain),
                (query_far, w_query),
                (key_far, w_key),
                (value_far, w_value),
                (gate_far, w_gate),
                (bias_far, bias),
                (parent_far, parent),
            )
        )
    ]
    for copy in copies:
        copy.start()
    heads = w_query.shape[1] // HEAD
    rows = heads * PROPS
    share = out.shape[1] - rows - PROPS
    copies[0].wait()
    flat = tokens[...].astype(F32)
    block = square_block(jnp.sum(flat * flat, axis=1, keepdims=True))
    copies[1].wait()
    scaled = (flat * gain[...]).astype(BF16)
    copies[2].wait()
    query = dot(scaled, w_query[...]).astype(BF16)
    for dest in range(INNER):
        for head in range(heads):
            out[dest, head * PROPS : (head + 1) * PROPS, :] = query[
                :, head * HEAD : (head + 1) * HEAD
            ]
        out[dest, rows + share :, :] = block
    slots = share // PROPS
    for which, weight in enumerate((w_key, w_value, w_gate)):
        copies[3 + which].wait()
        part = dot(scaled, weight[...]).astype(BF16)
        for head in range(heads):
            dest, slot = divmod(which * heads + head, slots)
            out[dest, rows + slot * PROPS : rows + (slot + 1) * PROPS, :] = part[
                :, head * HEAD : (head + 1) * HEAD
            ]
    for spare in range(3 * heads, INNER * slots):
        dest, slot = divmod(spare, slots)
        out[dest, rows + slot * PROPS : rows + (slot + 1) * PROPS, :] = jnp.zeros(
            (PROPS, HEAD), BF16
        )
    for copy in copies[6:]:
        copy.wait()


def add_up(parts):
    total = parts[0].astype(F32)
    for part in parts[1:]:
        total = total + part.astype(F32)
    return total


def forward_kernel(arrived, out):
    count = arrived.shape[1] - PROPS
    total = add_up([arrived[source] for source in range(INNER)])
    out[:count, :] = total[:count].astype(BF16)
    out[count:, :] = square_block(jnp.sum(total[count:], axis=1, keepdims=True))


def fetch_kernel(sums, keys_far, values_far, keys, values, sems):
    del sums
    copies = [
        pltpu.make_async_copy(keys_far, keys, sems.at[0]),
        pltpu.make_async_copy(values_far, values, sems.at[1]),
    ]
    for copy in copies:
        copy.start()
    for copy in copies:
        copy.wait()


def attend_kernel(
    prefix_len,
    accepted,
    bias,
    own,
    first_part,
    second_part,
    third_part,
    keys,
    values,
    out,
    query_out,
    limits,
):
    heads, ctx_dev, _ = keys.shape
    rows = heads * PROPS
    offset = prefix_len[0] + accepted[0] - lax.axis_index("kv") * ctx_dev
    first = jnp.minimum(jnp.maximum(offset, 0), ctx_dev - WINDOW)
    first = pl.multiple_of((first >> 4) << 4, PROPS)
    limits[0] = offset
    limits[1] = first
    total = add_up([own[...], first_part[...], second_part[...], third_part[...]])
    squares = jnp.sum(total[own.shape[0] - PROPS :], axis=1, keepdims=True)
    rscale = lax.rsqrt(squares / D + EPS)
    share = own.shape[0] - PROPS - rows
    for slot in range(share // PROPS):
        there = slice(rows + slot * PROPS, rows + (slot + 1) * PROPS)
        piece = (total[there] * rscale).astype(BF16)
        for dest in range(INNER):
            out[dest, there, :] = piece
    factor = HEAD ** (-0.5)
    live = iota((PROPS, ctx_dev), 1) < offset
    takes, keeps = [], []
    for head in range(heads):
        there = slice(head * PROPS, (head + 1) * PROPS)
        query = (total[there] * rscale).astype(BF16)
        query_out[there, :] = query
        scores = dot_t(query, keys[head]) * factor + bias[head]
        take, keep = log_sigmoids(scores)
        takes.append(take)
        keeps.append(jnp.where(live, keep, 0.0))
    keep = jnp.concatenate(keeps, axis=0)
    table = after_table(HEAD)
    beyond = jnp.zeros((rows, HEAD), F32)
    laters = []
    for chunk in reversed(range(ctx_dev // HEAD)):
        inside, whole = after_and_all(keep[:, chunk * HEAD : (chunk + 1) * HEAD], table)
        laters.append(inside + beyond)
        beyond = beyond + whole
    later = jnp.concatenate(laters[::-1], axis=1)
    rests = []
    for head in range(heads):
        there = slice(head * PROPS, (head + 1) * PROPS)
        weight = jnp.where(live, jnp.exp(takes[head] + later[there]), 0.0).astype(BF16)
        summed = dot(weight, values[head]).astype(BF16)
        for dest in range(INNER):
            out[dest, there, :] = summed
        rests.append(beyond[there])
    block = rest_block(rests)
    for dest in range(INNER):
        out[dest, rows + share :, :] = block


def merge_kernel(arrived, out, fresh):
    count = arrived.shape[0]
    rows = out.shape[0] - PROPS
    heads = rows // PROPS
    share = arrived.shape[1] - PROPS - rows
    for source in range(count):
        fresh[source * share : (source + 1) * share, :] = arrived[source, rows : rows + share, :]
    beyond = jnp.zeros((PROPS, HEAD), F32)
    factors = []
    for source in reversed(range(count)):
        factors.append(jnp.exp(beyond))
        beyond = beyond + rest_sums(arrived[source, rows + share :, :])
    factors = factors[::-1]
    for head in range(heads):
        there = slice(head * PROPS, (head + 1) * PROPS)
        total = jnp.zeros((PROPS, HEAD), F32)
        for source in range(count):
            total = total + factors[source][:, head : head + 1] * arrived[
                source, there, :
            ].astype(F32)
        out[there, :] = total.astype(BF16)
    out[rows:, :] = rest_block([beyond[:, head : head + 1] for head in range(heads)])


def tree_kernel(
    limits,
    bias,
    parent,
    fresh,
    query,
    keys,
    values,
    tree_out,
    tail_out,
    gate_out,
    keys_next,
    values_next,
    patches,
    masks,
    sems,
):
    heads = keys_next.shape[0]
    bulk = [
        pltpu.make_async_copy(keys, keys_next, sems.at[0]),
        pltpu.make_async_copy(values, values_next, sems.at[1]),
    ]
    for copy in bulk:
        copy.start()
    offset = limits[0]
    first = pl.multiple_of(limits[1], PROPS)
    source = first + iota((WINDOW, PROPS), 0) - offset
    picker = jnp.where(source == iota((WINDOW, PROPS), 1), 1.0, 0.0).astype(BF16)
    source = first + iota((WINDOW, HEAD), 0) - offset
    inside = (source >= 0) & (source < PROPS)
    copies = []
    for which, (cache, target) in enumerate(((keys, keys_next), (values, values_next))):
        for head in range(heads):
            start = (which * heads + head) * PROPS
            placed = dot(picker, fresh[start : start + PROPS, :])
            there = cache[head, pl.ds(first, WINDOW), :].astype(F32)
            patches[which, head] = jnp.where(inside, placed, there).astype(BF16)
        copies.append(
            pltpu.make_async_copy(
                patches.at[which], target.at[:, pl.ds(first, WINDOW), :], sems.at[2 + which]
            )
        )
    row = iota((PROPS, PROPS), 0)
    reach = jnp.zeros((PROPS, PROPS), jnp.int32)
    masks[0] = 0
    for index in range(1, PROPS):
        above = parent[index]
        mask = masks[above] | (1 << above)
        masks[index] = mask
        reach = jnp.where(row == index, mask, reach)
    family = ((reach >> iota((PROPS, PROPS), 1)) & 1) == 1
    factor = HEAD ** (-0.5)
    takes, keeps = [], []
    for head in range(heads):
        there = slice(head * PROPS, (head + 1) * PROPS)
        scores = dot_t(query[there, :], fresh[there, :]) * factor + bias[head]
        take, keep = log_sigmoids(scores)
        takes.append(take)
        keeps.append(jnp.where(family, keep, 0.0))
    later, tail = after_and_all(jnp.concatenate(keeps, axis=0), after_table(PROPS))
    tail_out[...] = tail
    for head in range(heads):
        there = slice(head * PROPS, (head + 1) * PROPS)
        weight = jnp.where(family, jnp.exp(takes[head] + later[there, :PROPS]), 0.0).astype(BF16)
        start = (heads + head) * PROPS
        tree_out[there, :] = dot(weight, fresh[start : start + PROPS, :])
    gate = fresh[2 * heads * PROPS : 3 * heads * PROPS, :].astype(F32)
    gate_out[...] = gate * jax.nn.sigmoid(gate)
    for before, copy in zip(bulk, copies):
        before.wait()
        copy.start()
    for copy in copies:
        copy.wait()


def finish_kernel(tree, tail, gate, w_out, own, first_part, second_part, third_part, out, mixin):
    parts = (own, first_part, second_part, third_part)
    outer = len(parts)
    rows = own.shape[0] - PROPS
    heads = rows // PROPS
    place = lax.axis_index("kv") // INNER
    spots = [lax.rem(place + outer - step, outer) for step in (0, *STEPS)]
    rests = [rest_sums(part[rows:, :]) for part in parts]
    beyonds = []
    for spot in spots:
        beyond = jnp.zeros((PROPS, HEAD), F32)
        for other, rest in zip(spots, rests):
            beyond = beyond + jnp.where(other > spot, rest, 0.0)
        beyonds.append(beyond)
    for head in range(heads):
        there = slice(head * PROPS, (head + 1) * PROPS)
        total = tree[there, :]
        for part, beyond in zip(parts, beyonds):
            total = total + jnp.exp(beyond[:, head : head + 1] + tail[there, :]) * part[
                there, :
            ].astype(F32)
        mixin[:, head * HEAD : (head + 1) * HEAD] = (total * gate[there, :]).astype(BF16)
    out[...] = dot_t(mixin[...], w_out[...]).astype(BF16)


def shaped(dims, dtype=BF16):
    return jax.ShapeDtypeStruct(dims, dtype)


def near(dims, dtype=BF16):
    return pltpu.VMEM(dims, dtype)


def held(value):
    return pltpu.with_memory_space_constraint(value, pltpu.VMEM)


def small(dims, dtype):
    return pltpu.SMEM(dims, dtype)


def far(value):
    return pltpu.with_memory_space_constraint(value, pltpu.HBM)


def kept(value):
    return pltpu.with_memory_space_constraint(value, pltpu.SMEM)


def local(
    tokens,
    norm_gain,
    w_query,
    w_key,
    w_value,
    w_gate,
    w_out,
    head_bias,
    cache_keys,
    cache_values,
    prefix_len,
    accepted,
    parent,
):
    columns, width = w_query.shape
    heads = width // HEAD
    rows = heads * PROPS
    share = -(-3 * heads // INNER) * PROPS
    sent = rows + share + PROPS
    keys = jnp.transpose(cache_keys[0], (1, 0, 2))
    values = jnp.transpose(cache_values[0], (1, 0, 2))

    pieces, bias, parents = pl.pallas_call(
        project_kernel,
        out_shape=(
            near((INNER, sent, HEAD)),
            small((heads,), F32),
            small((PROPS,), jnp.int32),
        ),
        in_specs=[ANY] * 8,
        out_specs=(VMEM, SMEM, SMEM),
        scratch_shapes=[
            pltpu.VMEM(tokens.shape[1:], BF16),
            pltpu.VMEM((1, columns), F32),
            *[pltpu.VMEM(w_query.shape, BF16)] * 4,
            pltpu.SemaphoreType.DMA((8,)),
        ],
        name="project",
        compiler_params=PARAMS,
    )(
        *(
            far(value)
            for value in (
                head_bias,
                parent[0],
                tokens[0],
                norm_gain[None],
                w_query,
                w_key,
                w_value,
                w_gate,
            )
        ),
    )
    bias, parents = kept(bias), kept(parents)
    pieces = pl.pallas_call(
        forward_kernel,
        out_shape=near((sent, HEAD)),
        in_specs=[VMEM],
        out_specs=VMEM,
        name="forward",
        compiler_params=PARAMS,
    )(exchange(pieces))
    keys, values = pl.pallas_call(
        fetch_kernel,
        out_shape=(near(keys.shape), near(values.shape)),
        in_specs=[ANY] * 3,
        out_specs=(VMEM, VMEM),
        scratch_shapes=[pltpu.SemaphoreType.DMA((2,))],
        name="fetch",
        compiler_params=PARAMS,
    )(held(pieces), far(keys), far(values))
    keys, values = held(keys), held(values)
    pieces, query, limits = pl.pallas_call(
        attend_kernel,
        out_shape=(
            near((INNER, sent, HEAD)),
            near((rows, HEAD)),
            small((2,), jnp.int32),
        ),
        in_specs=[SMEM] * 3 + [VMEM] * 6,
        out_specs=(VMEM, VMEM, SMEM),
        name="attend",
        compiler_params=PARAMS,
    )(
        prefix_len,
        accepted,
        bias,
        *shifted(pieces),
        keys,
        values,
    )
    pieces, fresh = pl.pallas_call(
        merge_kernel,
        out_shape=(near((rows + PROPS, HEAD)), near((INNER * share, HEAD))),
        in_specs=[VMEM],
        out_specs=(VMEM, VMEM),
        name="merge",
        compiler_params=PARAMS,
    )(exchange(pieces))
    parts = shifted(pieces)
    tree, tail, gate, keys_next, values_next = pl.pallas_call(
        tree_kernel,
        out_shape=(
            *[near((rows, HEAD), F32)] * 3,
            shaped(keys.shape),
            shaped(values.shape),
        ),
        in_specs=[SMEM] * 3 + [VMEM] * 4,
        out_specs=(VMEM, VMEM, VMEM, ANY, ANY),
        scratch_shapes=[
            pltpu.VMEM((2, heads, WINDOW, HEAD), BF16),
            pltpu.SMEM((PROPS,), jnp.int32),
            pltpu.SemaphoreType.DMA((4,)),
        ],
        name="tree",
        compiler_params=PARAMS,
    )(
        kept(limits),
        bias,
        parents,
        held(fresh),
        held(query),
        keys,
        values,
    )
    part_out = pl.pallas_call(
        finish_kernel,
        out_shape=near((PROPS, w_out.shape[1])),
        in_specs=[VMEM] * 8,
        out_specs=VMEM,
        scratch_shapes=[pltpu.VMEM((PROPS, heads * HEAD), BF16)],
        name="finish",
        compiler_params=PARAMS,
    )(held(tree), held(tail), held(gate), held(w_out.T), *parts)
    other = lax.ppermute(part_out, "tp", [(0, 1), (1, 0)])
    mixed = (part_out.astype(F32) + other.astype(F32)).astype(BF16)[None]
    return (
        mixed,
        jnp.transpose(keys_next, (1, 0, 2))[None],
        jnp.transpose(values_next, (1, 0, 2))[None],
    )


def solution(mesh):
    return jax.shard_map(
        local,
        mesh=mesh,
        in_specs=(
            P("dp", None, "kv"),
            P("kv"),
            P("kv", "tp"),
            P("kv", "tp"),
            P("kv", "tp"),
            P("kv", "tp"),
            P("tp", "kv"),
            P("tp"),
            P("dp", "kv", "tp", None),
            P("dp", "kv", "tp", None),
            P("dp"),
            P("dp"),
            P("dp", None),
        ),
        out_specs=(P("dp", None, "kv"), P("dp", "kv", "tp", None), P("dp", "kv", "tp", None)),
        check_vma=False,
    )
```

```python
import jax
import jax.numpy as jnp
from jax import lax
from jax.experimental import pallas as pl
from jax.experimental.pallas import tpu as pltpu
from jax.sharding import PartitionSpec as P

D = 2048
HEAD = 128
EPS = 1e-06
INNER = 8
PROPS = 16
WINDOW = 32
FIRST = (2, 3, 1)
LAST = (2, 1, 3)
F32 = jnp.float32
BF16 = jnp.bfloat16
VMEM = pl.BlockSpec(memory_space=pltpu.VMEM)
SMEM = pl.BlockSpec(memory_space=pltpu.SMEM)
ANY = pl.BlockSpec(memory_space=pl.ANY)
PARAMS = pltpu.CompilerParams(vmem_limit_bytes=16 * 2**20)


def exchange(pieces):
    outer = lax.axis_size("kv") // INNER
    groups = [[a * INNER + i for i in range(INNER)] for a in range(outer)]
    return held(lax.all_to_all(pieces, "kv", 0, 0, axis_index_groups=groups, tiled=True))


def shifted(value, steps):
    count = lax.axis_size("kv")
    parts = [value]
    for step in steps:
        pairs = [(spot, (spot + step * INNER) % count) for spot in range(count)]
        parts.append(lax.ppermute(value, "kv", pairs))
    return [held(part) for part in parts]


def iota(shape, dim):
    return lax.broadcasted_iota(jnp.int32, shape, dim)


def in_three(value):
    high = value.astype(BF16).astype(F32)
    rest = value - high
    middle = rest.astype(BF16).astype(F32)
    return high, middle, rest - middle


def dot(left, right):
    return jnp.dot(left, right, preferred_element_type=F32)


def dot_t(left, right):
    return lax.dot_general(left, right, (((1,), (1,)), ((), ())), preferred_element_type=F32)


def log_sigmoids(scores):
    soft = jnp.log1p(jnp.exp(-jnp.abs(scores)))
    return jnp.minimum(scores, 0.0) - soft, jnp.minimum(-scores, 0.0) - soft


def square_block(squares):
    lane = iota((PROPS, HEAD), 1)
    block = jnp.zeros((PROPS, HEAD), F32)
    for index, piece in enumerate(in_three(squares)):
        block = jnp.where(lane == index, piece, block)
    return block.astype(BF16)


def rest_block(rests):
    lane = iota((PROPS, HEAD), 1)
    block = jnp.zeros((PROPS, HEAD), F32)
    for index, rest in enumerate(rests):
        block = jnp.where(lane == index, rest, block)
    high, middle, low = in_three(block)
    block = high + pltpu.roll(middle, PROPS, 1) + pltpu.roll(low, 2 * PROPS, 1)
    return block.astype(BF16)


def rest_sums(block):
    block = block.astype(F32)
    return block + pltpu.roll(block, HEAD - PROPS, 1) + pltpu.roll(block, HEAD - 2 * PROPS, 1)


def after_table(width):
    row = iota((width, 2 * HEAD), 0)
    column = iota((width, 2 * HEAD), 1)
    return jnp.where((row > column) | (column >= HEAD), 1.0, 0.0).astype(BF16)


def after_and_all(values, table):
    high = values.astype(BF16)
    rest = values - high.astype(F32)
    middle = rest.astype(BF16)
    low = (rest - middle.astype(F32)).astype(BF16)
    sums = dot(high, table) + dot(middle, table) + dot(low, table)
    return sums[:, :HEAD], sums[:, HEAD:]


def project_kernel(
    bias_far,
    parent_far,
    tokens_far,
    gain_far,
    query_far,
    key_far,
    value_far,
    gate_far,
    out,
    bias,
    parent,
    tokens,
    gain,
    w_query,
    w_key,
    w_value,
    w_gate,
    sems,
):
    copies = [
        pltpu.make_async_copy(source, target, sems.at[index])
        for index, (source, target) in enumerate(
            (
                (tokens_far, tokens),
                (gain_far, gain),
                (query_far, w_query),
                (key_far, w_key),
                (value_far, w_value),
                (gate_far, w_gate),
                (bias_far, bias),
                (parent_far, parent),
            )
        )
    ]
    for copy in copies:
        copy.start()
    heads = w_query.shape[1] // HEAD
    rows = heads * PROPS
    share = out.shape[1] - rows - PROPS
    copies[0].wait()
    flat = tokens[...].astype(F32)
    block = square_block(jnp.sum(flat * flat, axis=1, keepdims=True))
    copies[1].wait()
    scaled = (flat * gain[...]).astype(BF16)
    copies[2].wait()
    query = dot(scaled, w_query[...]).astype(BF16)
    for dest in range(INNER):
        for head in range(heads):
            out[dest, head * PROPS : (head + 1) * PROPS, :] = query[
                :, head * HEAD : (head + 1) * HEAD
            ]
        out[dest, rows + share :, :] = block
    slots = share // PROPS
    for which, weight in enumerate((w_key, w_value, w_gate)):
        copies[3 + which].wait()
        part = dot(scaled, weight[...]).astype(BF16)
        for head in range(heads):
            dest, slot = divmod(which * heads + head, slots)
            out[dest, rows + slot * PROPS : rows + (slot + 1) * PROPS, :] = part[
                :, head * HEAD : (head + 1) * HEAD
            ]
    for spare in range(3 * heads, INNER * slots):
        dest, slot = divmod(spare, slots)
        out[dest, rows + slot * PROPS : rows + (slot + 1) * PROPS, :] = jnp.zeros(
            (PROPS, HEAD), BF16
        )
    for copy in copies[6:]:
        copy.wait()


def add_up(parts):
    total = parts[0].astype(F32)
    for part in parts[1:]:
        total = total + part.astype(F32)
    return total


def forward_kernel(arrived, out):
    count = arrived.shape[1] - PROPS
    total = add_up([arrived[source] for source in range(INNER)])
    out[:count, :] = total[:count].astype(BF16)
    out[count:, :] = square_block(jnp.sum(total[count:], axis=1, keepdims=True))


def fetch_kernel(sums, keys_far, values_far, keys, values, sems):
    del sums
    copies = [
        pltpu.make_async_copy(keys_far, keys, sems.at[0]),
        pltpu.make_async_copy(values_far, values, sems.at[1]),
    ]
    for copy in copies:
        copy.start()
    for copy in copies:
        copy.wait()


def attend_kernel(
    prefix_len,
    accepted,
    bias,
    own,
    first_part,
    second_part,
    third_part,
    keys,
    values,
    out,
    query_out,
    limits,
):
    heads, ctx_dev, _ = keys.shape
    rows = heads * PROPS
    offset = prefix_len[0] + accepted[0] - lax.axis_index("kv") * ctx_dev
    first = jnp.minimum(jnp.maximum(offset, 0), ctx_dev - WINDOW)
    first = pl.multiple_of((first >> 4) << 4, PROPS)
    limits[0] = offset
    limits[1] = first
    total = add_up([own[...], first_part[...], second_part[...], third_part[...]])
    squares = jnp.sum(total[own.shape[0] - PROPS :], axis=1, keepdims=True)
    rscale = lax.rsqrt(squares / D + EPS)
    share = own.shape[0] - PROPS - rows
    for slot in range(share // PROPS):
        there = slice(rows + slot * PROPS, rows + (slot + 1) * PROPS)
        piece = (total[there] * rscale).astype(BF16)
        for dest in range(INNER):
            out[dest, there, :] = piece
    factor = HEAD ** (-0.5)
    live = iota((PROPS, ctx_dev), 1) < offset
    takes, keeps = [], []
    for head in range(heads):
        there = slice(head * PROPS, (head + 1) * PROPS)
        query = (total[there] * rscale).astype(BF16)
        query_out[there, :] = query
        scores = dot_t(query, keys[head]) * factor + bias[head]
        take, keep = log_sigmoids(scores)
        takes.append(take)
        keeps.append(jnp.where(live, keep, 0.0))
    keep = jnp.concatenate(keeps, axis=0)
    table = after_table(HEAD)
    beyond = jnp.zeros((rows, HEAD), F32)
    laters = []
    for chunk in reversed(range(ctx_dev // HEAD)):
        inside, whole = after_and_all(keep[:, chunk * HEAD : (chunk + 1) * HEAD], table)
        laters.append(inside + beyond)
        beyond = beyond + whole
    later = jnp.concatenate(laters[::-1], axis=1)
    rests = []
    for head in range(heads):
        there = slice(head * PROPS, (head + 1) * PROPS)
        weight = jnp.where(live, jnp.exp(takes[head] + later[there]), 0.0).astype(BF16)
        summed = dot(weight, values[head]).astype(BF16)
        for dest in range(INNER):
            out[dest, there, :] = summed
        rests.append(beyond[there])
    block = rest_block(rests)
    for dest in range(INNER):
        out[dest, rows + share :, :] = block


def merge_kernel(arrived, out, fresh):
    count = arrived.shape[0]
    rows = out.shape[0] - PROPS
    heads = rows // PROPS
    share = arrived.shape[1] - PROPS - rows
    for source in range(count):
        fresh[source * share : (source + 1) * share, :] = arrived[source, rows : rows + share, :]
    beyond = jnp.zeros((PROPS, HEAD), F32)
    factors = []
    for source in reversed(range(count)):
        factors.append(jnp.exp(beyond))
        beyond = beyond + rest_sums(arrived[source, rows + share :, :])
    factors = factors[::-1]
    for head in range(heads):
        there = slice(head * PROPS, (head + 1) * PROPS)
        total = arrived[count - 1, there, :].astype(F32)
        for source in range(count - 1):
            total = total + factors[source][:, head : head + 1] * arrived[
                source, there, :
            ].astype(F32)
        out[there, :] = total.astype(BF16)
    out[rows:, :] = rest_block([beyond[:, head : head + 1] for head in range(heads)])


def tree_kernel(
    limits,
    bias,
    parent,
    fresh,
    query,
    keys,
    values,
    tree_out,
    tail_out,
    gate_out,
    keys_next,
    values_next,
    patches,
    masks,
    sems,
):
    heads = keys_next.shape[0]
    bulk = [
        pltpu.make_async_copy(keys, keys_next, sems.at[0]),
        pltpu.make_async_copy(values, values_next, sems.at[1]),
    ]
    for copy in bulk:
        copy.start()
    offset = limits[0]
    first = pl.multiple_of(limits[1], PROPS)
    source = first + iota((WINDOW, PROPS), 0) - offset
    picker = jnp.where(source == iota((WINDOW, PROPS), 1), 1.0, 0.0).astype(BF16)
    source = first + iota((WINDOW, HEAD), 0) - offset
    inside = (source >= 0) & (source < PROPS)
    copies = []
    for which, (cache, target) in enumerate(((keys, keys_next), (values, values_next))):
        for head in range(heads):
            start = (which * heads + head) * PROPS
            placed = dot(picker, fresh[start : start + PROPS, :])
            there = cache[head, pl.ds(first, WINDOW), :].astype(F32)
            patches[which, head] = jnp.where(inside, placed, there).astype(BF16)
        copies.append(
            pltpu.make_async_copy(
                patches.at[which], target.at[:, pl.ds(first, WINDOW), :], sems.at[2 + which]
            )
        )
    row = iota((PROPS, PROPS), 0)
    reach = jnp.zeros((PROPS, PROPS), jnp.int32)
    masks[0] = 0
    for index in range(1, PROPS):
        above = parent[index]
        mask = masks[above] | (1 << above)
        masks[index] = mask
        reach = jnp.where(row == index, mask, reach)
    family = ((reach >> iota((PROPS, PROPS), 1)) & 1) == 1
    factor = HEAD ** (-0.5)
    takes, keeps = [], []
    for head in range(heads):
        there = slice(head * PROPS, (head + 1) * PROPS)
        scores = dot_t(query[there, :], fresh[there, :]) * factor + bias[head]
        take, keep = log_sigmoids(scores)
        takes.append(take)
        keeps.append(jnp.where(family, keep, 0.0))
    later, tail = after_and_all(jnp.concatenate(keeps, axis=0), after_table(PROPS))
    tail_out[...] = jnp.exp(tail)
    for head in range(heads):
        there = slice(head * PROPS, (head + 1) * PROPS)
        weight = jnp.where(family, jnp.exp(takes[head] + later[there, :PROPS]), 0.0).astype(BF16)
        start = (heads + head) * PROPS
        tree_out[there, :] = dot(weight, fresh[start : start + PROPS, :])
    gate = fresh[2 * heads * PROPS : 3 * heads * PROPS, :].astype(F32)
    gate_out[...] = gate * jax.nn.sigmoid(gate)
    for before, copy in zip(bulk, copies):
        before.wait()
        copy.start()
    for copy in copies:
        copy.wait()


def finish_kernel(tree, tail, gate, w_out, own, first_part, second_part, third_part, out, mixin):
    parts = (own, first_part, second_part, third_part)
    outer = len(parts)
    rows = own.shape[0] - PROPS
    heads = rows // PROPS
    place = lax.axis_index("kv") // INNER
    spots = [lax.rem(place + outer - step, outer) for step in (0, *LAST)]
    rests = [rest_sums(part[rows:, :]) for part in parts]
    beyonds = []
    for spot in spots:
        beyond = jnp.zeros((PROPS, HEAD), F32)
        for other, rest in zip(spots, rests):
            beyond = beyond + jnp.where(other > spot, rest, 0.0)
        beyonds.append(jnp.exp(beyond))
    for head in range(heads):
        there = slice(head * PROPS, (head + 1) * PROPS)
        total = jnp.zeros((PROPS, HEAD), F32)
        for part, scale in zip(parts, beyonds):
            total = total + scale[:, head : head + 1] * part[there, :].astype(F32)
        total = tree[there, :] + total * tail[there, :]
        mixin[:, head * HEAD : (head + 1) * HEAD] = (total * gate[there, :]).astype(BF16)
    out[...] = dot_t(mixin[...], w_out[...]).astype(BF16)


def shaped(dims, dtype=BF16):
    return jax.ShapeDtypeStruct(dims, dtype)


def near(dims, dtype=BF16):
    return pltpu.VMEM(dims, dtype)


def held(value):
    return pltpu.with_memory_space_constraint(value, pltpu.VMEM)


def small(dims, dtype):
    return pltpu.SMEM(dims, dtype)


def far(value):
    return pltpu.with_memory_space_constraint(value, pltpu.HBM)


def kept(value):
    return pltpu.with_memory_space_constraint(value, pltpu.SMEM)


def local(
    tokens,
    norm_gain,
    w_query,
    w_key,
    w_value,
    w_gate,
    w_out,
    head_bias,
    cache_keys,
    cache_values,
    prefix_len,
    accepted,
    parent,
):
    columns, width = w_query.shape
    heads = width // HEAD
    rows = heads * PROPS
    share = -(-3 * heads // INNER) * PROPS
    sent = rows + share + PROPS
    keys = jnp.transpose(cache_keys[0], (1, 0, 2))
    values = jnp.transpose(cache_values[0], (1, 0, 2))

    pieces, bias, parents = pl.pallas_call(
        project_kernel,
        out_shape=(
            near((INNER, sent, HEAD)),
            small((heads,), F32),
            small((PROPS,), jnp.int32),
        ),
        in_specs=[ANY] * 8,
        out_specs=(VMEM, SMEM, SMEM),
        scratch_shapes=[
            pltpu.VMEM(tokens.shape[1:], BF16),
            pltpu.VMEM((1, columns), F32),
            *[pltpu.VMEM(w_query.shape, BF16)] * 4,
            pltpu.SemaphoreType.DMA((8,)),
        ],
        name="project",
        compiler_params=PARAMS,
    )(
        *(
            far(value)
            for value in (
                head_bias,
                parent[0],
                tokens[0],
                norm_gain[None],
                w_query,
                w_key,
                w_value,
                w_gate,
            )
        ),
    )
    bias, parents = kept(bias), kept(parents)
    pieces = pl.pallas_call(
        forward_kernel,
        out_shape=near((sent, HEAD)),
        in_specs=[VMEM],
        out_specs=VMEM,
        name="forward",
        compiler_params=PARAMS,
    )(exchange(pieces))
    keys, values = pl.pallas_call(
        fetch_kernel,
        out_shape=(near(keys.shape), near(values.shape)),
        in_specs=[ANY] * 3,
        out_specs=(VMEM, VMEM),
        scratch_shapes=[pltpu.SemaphoreType.DMA((2,))],
        name="fetch",
        compiler_params=PARAMS,
    )(held(pieces), far(keys), far(values))
    keys, values = held(keys), held(values)
    pieces, query, limits = pl.pallas_call(
        attend_kernel,
        out_shape=(
            near((INNER, sent, HEAD)),
            near((rows, HEAD)),
            small((2,), jnp.int32),
        ),
        in_specs=[SMEM] * 3 + [VMEM] * 6,
        out_specs=(VMEM, VMEM, SMEM),
        name="attend",
        compiler_params=PARAMS,
    )(
        prefix_len,
        accepted,
        bias,
        *shifted(pieces, FIRST),
        keys,
        values,
    )
    pieces, fresh = pl.pallas_call(
        merge_kernel,
        out_shape=(near((rows + PROPS, HEAD)), near((INNER * share, HEAD))),
        in_specs=[VMEM],
        out_specs=(VMEM, VMEM),
        name="merge",
        compiler_params=PARAMS,
    )(exchange(pieces))
    parts = shifted(pieces, LAST)
    tree, tail, gate, keys_next, values_next = pl.pallas_call(
        tree_kernel,
        out_shape=(
            *[near((rows, HEAD), F32)] * 3,
            shaped(keys.shape),
            shaped(values.shape),
        ),
        in_specs=[SMEM] * 3 + [VMEM] * 4,
        out_specs=(VMEM, VMEM, VMEM, ANY, ANY),
        scratch_shapes=[
            pltpu.VMEM((2, heads, WINDOW, HEAD), BF16),
            pltpu.SMEM((PROPS,), jnp.int32),
            pltpu.SemaphoreType.DMA((4,)),
        ],
        name="tree",
        compiler_params=PARAMS,
    )(
        kept(limits),
        bias,
        parents,
        held(fresh),
        held(query),
        keys,
        values,
    )
    part_out = pl.pallas_call(
        finish_kernel,
        out_shape=near((PROPS, w_out.shape[1])),
        in_specs=[VMEM] * 8,
        out_specs=VMEM,
        scratch_shapes=[pltpu.VMEM((PROPS, heads * HEAD), BF16)],
        name="finish",
        compiler_params=PARAMS,
    )(held(tree), held(tail), held(gate), held(w_out.T), *parts)
    other = lax.ppermute(part_out, "tp", [(0, 1), (1, 0)])
    mixed = (part_out.astype(F32) + other.astype(F32)).astype(BF16)[None]
    return (
        mixed,
        jnp.transpose(keys_next, (1, 0, 2))[None],
        jnp.transpose(values_next, (1, 0, 2))[None],
    )


def solution(mesh):
    return jax.shard_map(
        local,
        mesh=mesh,
        in_specs=(
            P("dp", None, "kv"),
            P("kv"),
            P("kv", "tp"),
            P("kv", "tp"),
            P("kv", "tp"),
            P("kv", "tp"),
            P("tp", "kv"),
            P("tp"),
            P("dp", "kv", "tp", None),
            P("dp", "kv", "tp", None),
            P("dp"),
            P("dp"),
            P("dp", None),
        ),
        out_specs=(P("dp", None, "kv"), P("dp", "kv", "tp", None), P("dp", "kv", "tp", None)),
        check_vma=False,
    )
```

```python
import jax
import jax.numpy as jnp
from jax import lax
from jax.experimental import pallas as pl
from jax.experimental.pallas import tpu as pltpu
from jax.sharding import PartitionSpec as P

D = 2048
HEAD = 128
EPS = 1e-06
INNER = 8
PROPS = 16
WINDOW = 32
FIRST = (2, 3, 1)
LAST = (2, 1, 3)
F32 = jnp.float32
BF16 = jnp.bfloat16
VMEM = pl.BlockSpec(memory_space=pltpu.VMEM)
SMEM = pl.BlockSpec(memory_space=pltpu.SMEM)
ANY = pl.BlockSpec(memory_space=pl.ANY)
PARAMS = pltpu.CompilerParams(vmem_limit_bytes=16 * 2**20)


def exchange(pieces):
    outer = lax.axis_size("kv") // INNER
    groups = [[a * INNER + i for i in range(INNER)] for a in range(outer)]
    return held(lax.all_to_all(pieces, "kv", 0, 0, axis_index_groups=groups, tiled=True))


def shifted(value, steps):
    count = lax.axis_size("kv")
    parts = [value]
    for step in steps:
        pairs = [(spot, (spot + step * INNER) % count) for spot in range(count)]
        parts.append(lax.ppermute(value, "kv", pairs))
    return [held(part) for part in parts]


def iota(shape, dim):
    return lax.broadcasted_iota(jnp.int32, shape, dim)


def in_three(value):
    high = value.astype(BF16).astype(F32)
    rest = value - high
    middle = rest.astype(BF16).astype(F32)
    return high, middle, rest - middle


def dot(left, right):
    return jnp.dot(left, right, preferred_element_type=F32)


def dot_t(left, right):
    return lax.dot_general(left, right, (((1,), (1,)), ((), ())), preferred_element_type=F32)


def log_sigmoids(scores):
    soft = jnp.log1p(jnp.exp(-jnp.abs(scores)))
    return jnp.minimum(scores, 0.0) - soft, jnp.minimum(-scores, 0.0) - soft


def square_block(squares):
    lane = iota((PROPS, HEAD), 1)
    block = jnp.zeros((PROPS, HEAD), F32)
    for index, piece in enumerate(in_three(squares)):
        block = jnp.where(lane == index, piece, block)
    return block.astype(BF16)


def rest_block(rests):
    lane = iota((PROPS, HEAD), 1)
    block = jnp.zeros((PROPS, HEAD), F32)
    for index, rest in enumerate(rests):
        block = jnp.where(lane == index, rest, block)
    high, middle, low = in_three(block)
    block = high + pltpu.roll(middle, PROPS, 1) + pltpu.roll(low, 2 * PROPS, 1)
    return block.astype(BF16)


def rest_sums(block):
    block = block.astype(F32)
    return block + pltpu.roll(block, HEAD - PROPS, 1) + pltpu.roll(block, HEAD - 2 * PROPS, 1)


def after_table(width):
    row = iota((width, 2 * HEAD), 0)
    column = iota((width, 2 * HEAD), 1)
    return jnp.where((row > column) | (column >= HEAD), 1.0, 0.0).astype(BF16)


def after_and_all(values, table):
    high = values.astype(BF16)
    rest = (values - high.astype(F32)).astype(BF16)
    sums = dot(high, table) + dot(rest, table)
    return sums[:, :HEAD], sums[:, HEAD:]


def project_kernel(
    bias_far,
    parent_far,
    tokens_far,
    gain_far,
    query_far,
    key_far,
    value_far,
    gate_far,
    out,
    bias,
    parent,
    tokens,
    gain,
    w_query,
    w_key,
    w_value,
    w_gate,
    sems,
):
    copies = [
        pltpu.make_async_copy(source, target, sems.at[index])
        for index, (source, target) in enumerate(
            (
                (tokens_far, tokens),
                (gain_far, gain),
                (query_far, w_query),
                (key_far, w_key),
                (value_far, w_value),
                (gate_far, w_gate),
                (bias_far, bias),
                (parent_far, parent),
            )
        )
    ]
    for copy in copies:
        copy.start()
    heads = w_query.shape[1] // HEAD
    rows = heads * PROPS
    share = out.shape[1] - rows - PROPS
    copies[0].wait()
    flat = tokens[...].astype(F32)
    block = square_block(jnp.sum(flat * flat, axis=1, keepdims=True))
    copies[1].wait()
    scaled = (flat * gain[...]).astype(BF16)
    copies[2].wait()
    query = dot(scaled, w_query[...]).astype(BF16)
    for dest in range(INNER):
        for head in range(heads):
            out[dest, head * PROPS : (head + 1) * PROPS, :] = query[
                :, head * HEAD : (head + 1) * HEAD
            ]
        out[dest, rows + share :, :] = block
    slots = share // PROPS
    for which, weight in enumerate((w_key, w_value, w_gate)):
        copies[3 + which].wait()
        part = dot(scaled, weight[...]).astype(BF16)
        for head in range(heads):
            dest, slot = divmod(which * heads + head, slots)
            out[dest, rows + slot * PROPS : rows + (slot + 1) * PROPS, :] = part[
                :, head * HEAD : (head + 1) * HEAD
            ]
    for spare in range(3 * heads, INNER * slots):
        dest, slot = divmod(spare, slots)
        out[dest, rows + slot * PROPS : rows + (slot + 1) * PROPS, :] = jnp.zeros(
            (PROPS, HEAD), BF16
        )
    for copy in copies[6:]:
        copy.wait()


def add_up(parts):
    total = parts[0].astype(F32)
    for part in parts[1:]:
        total = total + part.astype(F32)
    return total


def forward_kernel(arrived, out):
    count = arrived.shape[1] - PROPS
    total = add_up([arrived[source] for source in range(INNER)])
    out[:count, :] = total[:count].astype(BF16)
    out[count:, :] = square_block(jnp.sum(total[count:], axis=1, keepdims=True))


def fetch_kernel(sums, keys_far, values_far, keys, values, sems):
    del sums
    copies = [
        pltpu.make_async_copy(keys_far, keys, sems.at[0]),
        pltpu.make_async_copy(values_far, values, sems.at[1]),
    ]
    for copy in copies:
        copy.start()
    for copy in copies:
        copy.wait()


def attend_kernel(
    prefix_len,
    accepted,
    bias,
    own,
    first_part,
    second_part,
    third_part,
    keys,
    values,
    out,
    query_out,
    limits,
):
    heads, ctx_dev, _ = keys.shape
    rows = heads * PROPS
    offset = prefix_len[0] + accepted[0] - lax.axis_index("kv") * ctx_dev
    first = jnp.minimum(jnp.maximum(offset, 0), ctx_dev - WINDOW)
    first = pl.multiple_of((first >> 4) << 4, PROPS)
    limits[0] = offset
    limits[1] = first
    total = add_up([own[...], first_part[...], second_part[...], third_part[...]])
    squares = jnp.sum(total[own.shape[0] - PROPS :], axis=1, keepdims=True)
    rscale = lax.rsqrt(squares / D + EPS)
    share = own.shape[0] - PROPS - rows
    for slot in range(share // PROPS):
        there = slice(rows + slot * PROPS, rows + (slot + 1) * PROPS)
        piece = (total[there] * rscale).astype(BF16)
        for dest in range(INNER):
            out[dest, there, :] = piece
    factor = HEAD ** (-0.5)
    live = iota((PROPS, ctx_dev), 1) < offset
    takes, keeps = [], []
    for head in range(heads):
        there = slice(head * PROPS, (head + 1) * PROPS)
        query = (total[there] * rscale).astype(BF16)
        query_out[there, :] = query
        scores = dot_t(query, keys[head]) * factor + bias[head]
        take, keep = log_sigmoids(scores)
        takes.append(take)
        keeps.append(jnp.where(live, keep, 0.0))
    keep = jnp.concatenate(keeps, axis=0)
    table = after_table(HEAD)
    beyond = jnp.zeros((rows, HEAD), F32)
    laters = []
    for chunk in reversed(range(ctx_dev // HEAD)):
        inside, whole = after_and_all(keep[:, chunk * HEAD : (chunk + 1) * HEAD], table)
        laters.append(inside + beyond)
        beyond = beyond + whole
    later = jnp.concatenate(laters[::-1], axis=1)
    rests = []
    for head in range(heads):
        there = slice(head * PROPS, (head + 1) * PROPS)
        weight = jnp.where(live, jnp.exp(takes[head] + later[there]), 0.0).astype(BF16)
        summed = dot(weight, values[head]).astype(BF16)
        for dest in range(INNER):
            out[dest, there, :] = summed
        rests.append(beyond[there])
    block = rest_block(rests)
    for dest in range(INNER):
        out[dest, rows + share :, :] = block


def merge_kernel(arrived, out, fresh):
    count = arrived.shape[0]
    rows = out.shape[0] - PROPS
    heads = rows // PROPS
    share = arrived.shape[1] - PROPS - rows
    for source in range(count):
        fresh[source * share : (source + 1) * share, :] = arrived[source, rows : rows + share, :]
    beyond = jnp.zeros((PROPS, HEAD), F32)
    factors = []
    for source in reversed(range(count)):
        factors.append(jnp.exp(beyond))
        beyond = beyond + rest_sums(arrived[source, rows + share :, :])
    factors = factors[::-1]
    for head in range(heads):
        there = slice(head * PROPS, (head + 1) * PROPS)
        total = arrived[count - 1, there, :].astype(F32)
        for source in range(count - 1):
            total = total + factors[source][:, head : head + 1] * arrived[
                source, there, :
            ].astype(F32)
        out[there, :] = total.astype(BF16)
    out[rows:, :] = rest_block([beyond[:, head : head + 1] for head in range(heads)])


def tree_kernel(
    limits,
    bias,
    parent,
    fresh,
    query,
    keys,
    values,
    tree_out,
    tail_out,
    gate_out,
    keys_next,
    values_next,
    patches,
    masks,
    sems,
):
    heads = keys_next.shape[0]
    bulk = [
        pltpu.make_async_copy(keys, keys_next, sems.at[0]),
        pltpu.make_async_copy(values, values_next, sems.at[1]),
    ]
    for copy in bulk:
        copy.start()
    offset = limits[0]
    first = pl.multiple_of(limits[1], PROPS)
    source = first + iota((WINDOW, PROPS), 0) - offset
    picker = jnp.where(source == iota((WINDOW, PROPS), 1), 1.0, 0.0).astype(BF16)
    source = first + iota((WINDOW, HEAD), 0) - offset
    inside = (source >= 0) & (source < PROPS)
    copies = []
    for which, (cache, target) in enumerate(((keys, keys_next), (values, values_next))):
        for head in range(heads):
            start = (which * heads + head) * PROPS
            placed = dot(picker, fresh[start : start + PROPS, :])
            there = cache[head, pl.ds(first, WINDOW), :].astype(F32)
            patches[which, head] = jnp.where(inside, placed, there).astype(BF16)
        copies.append(
            pltpu.make_async_copy(
                patches.at[which], target.at[:, pl.ds(first, WINDOW), :], sems.at[2 + which]
            )
        )
    row = iota((PROPS, PROPS), 0)
    reach = jnp.zeros((PROPS, PROPS), jnp.int32)
    masks[0] = 0
    for index in range(1, PROPS):
        above = parent[index]
        mask = masks[above] | (1 << above)
        masks[index] = mask
        reach = jnp.where(row == index, mask, reach)
    family = ((reach >> iota((PROPS, PROPS), 1)) & 1) == 1
    factor = HEAD ** (-0.5)
    takes, keeps = [], []
    for head in range(heads):
        there = slice(head * PROPS, (head + 1) * PROPS)
        scores = dot_t(query[there, :], fresh[there, :]) * factor + bias[head]
        take, keep = log_sigmoids(scores)
        takes.append(take)
        keeps.append(jnp.where(family, keep, 0.0))
    later, tail = after_and_all(jnp.concatenate(keeps, axis=0), after_table(PROPS))
    tail_out[...] = jnp.exp(tail)
    for head in range(heads):
        there = slice(head * PROPS, (head + 1) * PROPS)
        weight = jnp.where(family, jnp.exp(takes[head] + later[there, :PROPS]), 0.0).astype(BF16)
        start = (heads + head) * PROPS
        tree_out[there, :] = dot(weight, fresh[start : start + PROPS, :])
    gate = fresh[2 * heads * PROPS : 3 * heads * PROPS, :].astype(F32)
    gate_out[...] = gate * jax.nn.sigmoid(gate)
    for before, copy in zip(bulk, copies):
        before.wait()
        copy.start()
    for copy in copies:
        copy.wait()


def finish_kernel(tree, tail, gate, w_out, own, first_part, second_part, third_part, out, mixin):
    parts = (own, first_part, second_part, third_part)
    outer = len(parts)
    rows = own.shape[0] - PROPS
    heads = rows // PROPS
    place = lax.axis_index("kv") // INNER
    spots = [lax.rem(place + outer - step, outer) for step in (0, *LAST)]
    rests = [rest_sums(part[rows:, :]) for part in parts]
    beyonds = []
    for spot in spots:
        beyond = jnp.zeros((PROPS, HEAD), F32)
        for other, rest in zip(spots, rests):
            beyond = beyond + jnp.where(other > spot, rest, 0.0)
        beyonds.append(jnp.exp(beyond))
    for head in range(heads):
        there = slice(head * PROPS, (head + 1) * PROPS)
        total = jnp.zeros((PROPS, HEAD), F32)
        for part, scale in zip(parts, beyonds):
            total = total + scale[:, head : head + 1] * part[there, :].astype(F32)
        total = tree[there, :] + total * tail[there, :]
        mixin[:, head * HEAD : (head + 1) * HEAD] = (total * gate[there, :]).astype(BF16)
    out[...] = dot_t(mixin[...], w_out[...]).astype(BF16)


def shaped(dims, dtype=BF16):
    return jax.ShapeDtypeStruct(dims, dtype)


def near(dims, dtype=BF16):
    return pltpu.VMEM(dims, dtype)


def held(value):
    return pltpu.with_memory_space_constraint(value, pltpu.VMEM)


def small(dims, dtype):
    return pltpu.SMEM(dims, dtype)


def far(value):
    return pltpu.with_memory_space_constraint(value, pltpu.HBM)


def kept(value):
    return pltpu.with_memory_space_constraint(value, pltpu.SMEM)


def local(
    tokens,
    norm_gain,
    w_query,
    w_key,
    w_value,
    w_gate,
    w_out,
    head_bias,
    cache_keys,
    cache_values,
    prefix_len,
    accepted,
    parent,
):
    columns, width = w_query.shape
    heads = width // HEAD
    rows = heads * PROPS
    share = -(-3 * heads // INNER) * PROPS
    sent = rows + share + PROPS
    keys = jnp.transpose(cache_keys[0], (1, 0, 2))
    values = jnp.transpose(cache_values[0], (1, 0, 2))

    pieces, bias, parents = pl.pallas_call(
        project_kernel,
        out_shape=(
            near((INNER, sent, HEAD)),
            small((heads,), F32),
            small((PROPS,), jnp.int32),
        ),
        in_specs=[ANY] * 8,
        out_specs=(VMEM, SMEM, SMEM),
        scratch_shapes=[
            pltpu.VMEM(tokens.shape[1:], BF16),
            pltpu.VMEM((1, columns), F32),
            *[pltpu.VMEM(w_query.shape, BF16)] * 4,
            pltpu.SemaphoreType.DMA((8,)),
        ],
        name="project",
        compiler_params=PARAMS,
    )(
        *(
            far(value)
            for value in (
                head_bias,
                parent[0],
                tokens[0],
                norm_gain[None],
                w_query,
                w_key,
                w_value,
                w_gate,
            )
        ),
    )
    bias, parents = kept(bias), kept(parents)
    pieces = pl.pallas_call(
        forward_kernel,
        out_shape=near((sent, HEAD)),
        in_specs=[VMEM],
        out_specs=VMEM,
        name="forward",
        compiler_params=PARAMS,
    )(exchange(pieces))
    keys, values = pl.pallas_call(
        fetch_kernel,
        out_shape=(near(keys.shape), near(values.shape)),
        in_specs=[ANY] * 3,
        out_specs=(VMEM, VMEM),
        scratch_shapes=[pltpu.SemaphoreType.DMA((2,))],
        name="fetch",
        compiler_params=PARAMS,
    )(held(pieces), far(keys), far(values))
    keys, values = held(keys), held(values)
    pieces, query, limits = pl.pallas_call(
        attend_kernel,
        out_shape=(
            near((INNER, sent, HEAD)),
            near((rows, HEAD)),
            small((2,), jnp.int32),
        ),
        in_specs=[SMEM] * 3 + [VMEM] * 6,
        out_specs=(VMEM, VMEM, SMEM),
        name="attend",
        compiler_params=PARAMS,
    )(
        prefix_len,
        accepted,
        bias,
        *shifted(pieces, FIRST),
        keys,
        values,
    )
    pieces, fresh = pl.pallas_call(
        merge_kernel,
        out_shape=(near((rows + PROPS, HEAD)), near((INNER * share, HEAD))),
        in_specs=[VMEM],
        out_specs=(VMEM, VMEM),
        name="merge",
        compiler_params=PARAMS,
    )(exchange(pieces))
    parts = shifted(pieces, LAST)
    tree, tail, gate, keys_next, values_next = pl.pallas_call(
        tree_kernel,
        out_shape=(
            *[near((rows, HEAD), F32)] * 3,
            shaped(keys.shape),
            shaped(values.shape),
        ),
        in_specs=[SMEM] * 3 + [VMEM] * 4,
        out_specs=(VMEM, VMEM, VMEM, ANY, ANY),
        scratch_shapes=[
            pltpu.VMEM((2, heads, WINDOW, HEAD), BF16),
            pltpu.SMEM((PROPS,), jnp.int32),
            pltpu.SemaphoreType.DMA((4,)),
        ],
        name="tree",
        compiler_params=PARAMS,
    )(
        kept(limits),
        bias,
        parents,
        held(fresh),
        held(query),
        keys,
        values,
    )
    part_out = pl.pallas_call(
        finish_kernel,
        out_shape=near((PROPS, w_out.shape[1])),
        in_specs=[VMEM] * 8,
        out_specs=VMEM,
        scratch_shapes=[pltpu.VMEM((PROPS, heads * HEAD), BF16)],
        name="finish",
        compiler_params=PARAMS,
    )(held(tree), held(tail), held(gate), held(w_out.T), *parts)
    other = lax.ppermute(part_out, "tp", [(0, 1), (1, 0)])
    mixed = (part_out.astype(F32) + other.astype(F32)).astype(BF16)[None]
    return (
        mixed,
        jnp.transpose(keys_next, (1, 0, 2))[None],
        jnp.transpose(values_next, (1, 0, 2))[None],
    )


def solution(mesh):
    return jax.shard_map(
        local,
        mesh=mesh,
        in_specs=(
            P("dp", None, "kv"),
            P("kv"),
            P("kv", "tp"),
            P("kv", "tp"),
            P("kv", "tp"),
            P("kv", "tp"),
            P("tp", "kv"),
            P("tp"),
            P("dp", "kv", "tp", None),
            P("dp", "kv", "tp", None),
            P("dp"),
            P("dp"),
            P("dp", None),
        ),
        out_specs=(P("dp", None, "kv"), P("dp", "kv", "tp", None), P("dp", "kv", "tp", None)),
        check_vma=False,
    )
```
